32 devices in a mesh: grp: 2 (over x), fs: 4 (over z), tp: 4 (over y, core).
Axes of the slice: x: 2, y: 2, z: 4, core: 2. Of those that a mesh axis runs over, the one named last changes fastest.
Arguments:
- tokens: bfloat16 [2048, 2048], P(('grp', 'fs'), 'tp'), parts along dimension 0, may hold values from -12 to 12
- gain_first: float32 [2048], P('tp'), may hold values from 0.1 to 1.9
- gate_first: float32 [2048, 5632], P('fs', 'tp'), may hold values from -0.125 to 0.125
- gate_scale_first: float32 [5632], P('tp'), may hold values from 0.5 to 2
- up_first: float32 [2048, 5632], P('fs', 'tp'), may hold values from -0.125 to 0.125
- up_scale_first: float32 [5632], P('tp'), may hold values from 0.5 to 2
- down_first: float32 [5632, 2048], P('tp', 'fs'), may hold values from -0.078125 to 0.078125
- down_scale_first: float32 [2048], P('tp'), may hold values from 0.5 to 2
- gain_second: float32 [2048], P('tp'), may hold values from 0.1 to 1.9
- gate_second: float32 [2048, 5632], P('fs', 'tp'), may hold values from -0.125 to 0.125
- gate_scale_second: float32 [5632], P('tp'), may hold values from 0.5 to 2
- up_second: float32 [2048, 5632], P('fs', 'tp'), may hold values from -0.125 to 0.125
- up_scale_second: float32 [5632], P('tp'), may hold values from 0.5 to 2
- down_second: float32 [5632, 2048], P('tp', 'fs'), may hold values from -0.078125 to 0.078125
- down_scale_second: float32 [2048], P('tp'), may hold values from 0.5 to 2
Outputs:
- stream_out: bfloat16 [2048, 2048], P(('grp', 'fs'), 'tp'), parts along dimension 0
The draws below stay inside these ranges and needn't reach their ends.
There are 2 independent parts, one for each index of `grp`. The reference program is written for one: setup_inputs(seed, part) draws one part's arguments, and reference() takes and returns one part's arrays. A program takes and returns all parts, laid end to end along the dimension named above; an argument that names none is the same for every part. Nothing has to cross between parts.
All inputs are finite; a program needn't handle non-finite values.
Results may differ from the reference program's by a relative error of at most 0.028.
Values may be sent and summed in bfloat16 or wider, within the bound.
A program may use at most 128 MiB of HBM per device.

```python
import math
import jax
import jax.numpy as jnp
from jax import lax

D = 2048
FF = 5632
TOKENS = 1024
N_TP = 4


def draw_tokens(key, part):
    keys = jax.random.split(key, 7)
    column = jnp.arange(D, dtype=jnp.float32)
    place = (column + 0.5) * (2.0 / D) - 1.0
    flip = jnp.where(jax.random.uniform(keys[0], (TOKENS, 1), jnp.float32) < 0.5, -1.0, 1.0)
    tilt = flip * jax.random.uniform(keys[1], (TOKENS, 1), jnp.float32, 0.6, 1.0)
    rough = jnp.exp(jax.random.uniform(keys[2], (1, D), jnp.float32, -0.7, 0.7))
    dense = jnp.exp(tilt * place[None, :] * math.log(2.0)) * rough
    share = jnp.exp(jax.random.uniform(keys[3], (TOKENS, 1), jnp.float32, math.log(0.02), 0.0))
    center = jax.random.uniform(keys[4], (TOKENS, 1), jnp.float32, 0.0, 1.0) * D
    width = jnp.exp(jax.random.uniform(keys[5], (TOKENS, 1), jnp.float32, 0.0, math.log(3.0)))
    distance = jnp.abs(column[None, :] - center)
    distance = jnp.minimum(distance, D - distance)
    band = 4.0 * jnp.exp(-0.5 * jnp.square(distance / width))
    amplitude = share * dense + band
    values = jax.random.normal(keys[6], (TOKENS, D), jnp.float32) * amplitude
    return jnp.clip(values, -12.0, 12.0).astype(jnp.bfloat16)


def shard_levels(stream_key, dims, cuts, smallest, top_value):
    factor_of = 1.0
    for dim, parts in cuts:
        draws = jax.random.uniform(jax.random.fold_in(jax.random.fold_in(stream_key, 6), dim), (parts,), jnp.float32, smallest / len(cuts), top_value / len(cuts))
        factor_of = factor_of * jnp.repeat(jnp.exp(draws), dims[dim] // parts).reshape((-1,) + (1,) * (len(dims) - 1 - dim))
    return factor_of


def gaussian(stream_key, dims, spread, reach, shards=(), held_as=jnp.bfloat16):
    entries = jax.random.normal(stream_key, dims, jnp.float32) * spread
    if len(shards) > 0:
        entries = shard_levels(stream_key, dims, shards, -0.22, 0.18) * entries
    return jnp.clip(entries, min=-reach, max=reach).astype(held_as)


def setup_inputs(seed: int = 0, part: int = 0) -> dict:
    streams_of = jax.random.split(jax.random.key(seed), 16)
    own_keys = jax.random.split(jax.random.fold_in(streams_of[15], part), 16)
    return {
        "tokens": draw_tokens(jax.random.fold_in(jax.random.fold_in(streams_of[15], part), 71), part),
        "gain_first": jnp.clip(1.0 + 0.18 * jax.random.normal(streams_of[1], (D,), jnp.float32), 0.1, 1.9),
        "gate_first": gaussian(streams_of[2], (D, FF), D ** -0.5, 0.125, ((0, 4), (1, 4)), jnp.float32),
        "gate_scale_first": jnp.clip(jnp.exp(math.log(2.0) - 1.3862944 * jax.random.uniform(streams_of[3], (FF,), jnp.float32) ** shard_levels(streams_of[3], (FF,), ((0, 4),), -0.2, 0.2)), 0.5, 2.0),
        "up_first": gaussian(streams_of[4], (D, FF), D ** -0.5, 0.125, ((0, 4), (1, 4)), jnp.float32),
        "up_scale_first": jnp.clip(jnp.exp(math.log(2.0) - 1.3862944 * jax.random.uniform(streams_of[5], (FF,), jnp.float32) ** shard_levels(streams_of[5], (FF,), ((0, 4),), -0.2, 0.2)), 0.5, 2.0),
        "down_first": gaussian(streams_of[6], (FF, D), FF ** -0.5, 0.078125, ((0, 4), (1, 4)), jnp.float32),
        "down_scale_first": jnp.clip(jnp.exp(math.log(2.0) - 1.3862944 * jax.random.uniform(streams_of[7], (D,), jnp.float32) ** shard_levels(streams_of[7], (D,), ((0, 4),), -0.2, 0.2)), 0.5, 2.0),
        "gain_second": jnp.clip(1.0 + 0.18 * jax.random.normal(streams_of[8], (D,), jnp.float32), 0.1, 1.9),
        "gate_second": gaussian(streams_of[9], (D, FF), D ** -0.5, 0.125, ((0, 4), (1, 4)), jnp.float32),
        "gate_scale_second": jnp.clip(jnp.exp(math.log(2.0) - 1.3862944 * jax.random.uniform(streams_of[10], (FF,), jnp.float32) ** shard_levels(streams_of[10], (FF,), ((0, 4),), -0.2, 0.2)), 0.5, 2.0),
        "up_second": gaussian(streams_of[11], (D, FF), D ** -0.5, 0.125, ((0, 4), (1, 4)), jnp.float32),
        "up_scale_second": jnp.clip(jnp.exp(math.log(2.0) - 1.3862944 * jax.random.uniform(streams_of[12], (FF,), jnp.float32) ** shard_levels(streams_of[12], (FF,), ((0, 4),), -0.2, 0.2)), 0.5, 2.0),
        "down_second": gaussian(streams_of[13], (FF, D), FF ** -0.5, 0.078125, ((0, 4), (1, 4)), jnp.float32),
        "down_scale_second": jnp.clip(jnp.exp(math.log(2.0) - 1.3862944 * jax.random.uniform(streams_of[14], (D,), jnp.float32) ** shard_levels(streams_of[14], (D,), ((0, 4),), -0.2, 0.2)), 0.5, 2.0),
    }


epsilon = 1e-06

def down_total(hidden, down_bf16):
    block = FF // N_TP
    hidden_blocks = hidden.reshape(TOKENS, N_TP, block).transpose(1, 0, 2)
    weight_blocks = down_bf16.reshape(N_TP, block, D)

    def step(total, pair):
        partial_value = jnp.dot(pair[0], pair[1], preferred_element_type=jnp.float32).astype(jnp.bfloat16)
        partial_value = lax.optimization_barrier(partial_value)
        return (total + partial_value.astype(jnp.float32), None)
    total, _ = lax.scan(step, jnp.zeros((TOKENS, D), jnp.float32), (hidden_blocks, weight_blocks))
    return total

def block_apply(stream, gain, gate_w, gate_s, up_w, up_s, down_w, down_s):
    values = stream.astype(jnp.float32)
    mean_sq = lax.optimization_barrier(jnp.mean(values * values, axis=1, keepdims=True))
    normed = (values * lax.rsqrt(mean_sq + epsilon) * gain).astype(jnp.bfloat16)
    gate = jnp.dot(normed, gate_w.astype(jnp.bfloat16), preferred_element_type=jnp.float32) * gate_s
    up = jnp.dot(normed, up_w.astype(jnp.bfloat16), preferred_element_type=jnp.float32) * up_s
    hidden = (jax.nn.silu(gate) * up).astype(jnp.bfloat16)
    total = down_total(hidden, down_w.astype(jnp.bfloat16)) * down_s
    return (values + 0.5 * total).astype(jnp.bfloat16)

def reference(tokens, gain_first, gate_first, gate_scale_first, up_first, up_scale_first, down_first, down_scale_first, gain_second, gate_second, gate_scale_second, up_second, up_scale_second, down_second, down_scale_second):
    middle = block_apply(tokens, gain_first, gate_first, gate_scale_first, up_first, up_scale_first, down_first, down_scale_first)
    return block_apply(middle, gain_second, gate_second, gate_scale_second, up_second, up_scale_second, down_second, down_scale_second)
```

```python
import functools

import jax
import jax.numpy as jnp
from jax import lax
from jax.experimental import pallas as pl
from jax.experimental.pallas import tpu as pltpu
from jax.sharding import PartitionSpec as P

MESH = pl.DeviceIdType.MESH
LANES = 128

epsilon = 1e-06


def normalize(stream, gain):
    values = stream.astype(jnp.float32)
    totals = lax.psum(jnp.sum(values * values, axis=1), "tp")
    width = values.shape[1] * lax.axis_size("tp")
    normed = (values * lax.rsqrt(totals / width + epsilon)[:, None] * gain).astype(jnp.bfloat16)
    return values, lax.all_gather(normed, "tp", axis=1, tiled=True)


def gathered_block(stream, gain, gate_w, gate_s, up_w, up_s, down_w, down_s):
    values, whole = normalize(stream, gain)

    def project(weight, scale):
        rows = lax.all_gather(weight.astype(jnp.bfloat16), "fs", axis=0, tiled=True)
        return jnp.dot(whole, rows, preferred_element_type=jnp.float32) * scale

    hidden = (jax.nn.silu(project(gate_w, gate_s)) * project(up_w, up_s)).astype(jnp.bfloat16)
    columns = lax.all_gather(down_w.astype(jnp.bfloat16), "fs", axis=1, tiled=True)
    terms = jnp.dot(hidden, columns, preferred_element_type=jnp.float32).astype(jnp.bfloat16)
    summed = lax.psum_scatter(terms, "tp", scatter_dimension=1, tiled=True).astype(jnp.float32)
    return (values + 0.5 * summed * down_s).astype(jnp.bfloat16)


def body_gather(tokens, *rest):
    middle = gathered_block(tokens, *rest[:7])
    return gathered_block(middle, *rest[7:])


def both_blocks(n_fs, n_tp, tiles, *refs):
    (tokens, gains, scales, down_scales), refs = refs[:4], refs[4:]
    weights, out, refs = refs[:6], refs[6], refs[7:]
    (
        wide_gate, wide_up, wide_down, all_gains,
        cols_0, cols_1, rows_0, rows_1, gu_0, gu_1, dn_0, dn_1, x_0, x_1, normed, hidden,
        core_out, from_core_0, from_core_1, y_out, from_y_0, from_y_1,
        z_out, from_left_0, from_left_1, from_right_0, from_right_1, total, kept,
        load_sem, gain_send, gain_recv,
        ag_zs, ag_zr, ag_ys, ag_yr, ag_cs, ag_cr,
        gu_zs, gu_zr, gu_xs, gu_xr, dn_zs, dn_zr, dn_xs, dn_xr,
        rs_cs, rs_cr, rs_ys, rs_yr, rs_zs, rs_lr, rs_rr,
    ) = refs
    cols, rows, gu, dn, x = (cols_0, cols_1), (rows_0, rows_1), (gu_0, gu_1), (dn_0, dn_1), (x_0, x_1)
    from_core, from_y = (from_core_0, from_core_1), (from_y_0, from_y_1)
    from_left, from_right = (from_left_0, from_left_1), (from_right_0, from_right_1)

    grp, fs, tp = lax.axis_index("grp"), lax.axis_index("fs"), lax.axis_index("tp")
    core, chip = lax.rem(tp, 2), lax.div(tp, 2)
    partner, other_core, across = {"grp": 1 - grp}, {"tp": tp + 1 - 2 * core}, {"tp": lax.rem(tp + 2, n_tp)}
    far_tp = lax.rem(tp + 2, n_tp)
    last = n_fs - 1
    base = -(-tiles // n_fs)
    short = n_fs * base - tiles
    bf, f32 = jnp.bfloat16, jnp.float32

    def first_tile(dev):
        even = jnp.minimum(dev, short)
        odd = jnp.maximum(dev - (n_fs - short), 0)
        return dev * base - (1 - core) * even - core * odd

    def has_last(dev):
        return first_tile(dev + 1) - first_tile(dev) == base

    def peer(d):
        return lax.rem(fs + d, n_fs)

    def origin(d):
        return lax.rem(fs + n_fs - d, n_fs)

    def remote(src, dst, sends, recvs, device):
        return pltpu.make_async_remote_copy(
            src_ref=src, dst_ref=dst, send_sem=sends, recv_sem=recvs, device_id=device, device_id_type=MESH
        )

    def when(cond, fn):
        if cond is None:
            fn()
        else:
            pl.when(cond)(fn)

    def gu_cond(i, dev):
        return has_last(dev) if i % base == base - 1 and short else None

    def gu_z(b, i):
        d, n = 1 + i // base, i % base
        src = cols[b].at[first_tile(peer(d)) + n, grp]
        return remote(src, gu[b].at[n, fs, grp], gu_zs.at[b, i], gu_zr.at[b, i], {"fs": peer(d)})

    def gu_x(b, i):
        d, n = 1 + i // base, i % base
        block = gu[b].at[n, origin(d), grp]
        return remote(block, block, gu_xs.at[b, i], gu_xr.at[b, i], partner)

    def gu_landed(b, i):
        d, n = 1 + i // base, i % base
        block = gu[b].at[n, origin(d), grp]
        return remote(block, block, gu_zs.at[b, i], gu_zr.at[b, i], {"fs": origin(d)})

    def dn_part(i):
        return pl.ds(0, base - 1) if i % 2 == 0 else pl.ds(base - 1, 1)

    def dn_cond(i, dev):
        return has_last(dev) if i % 2 == 1 and short else None

    def dn_z(b, i):
        d = 1 + i // 2
        start = first_tile(peer(d))
        src = pl.ds(start, base - 1) if i % 2 == 0 else pl.ds(start + base - 1, 1)
        dst = dn[b].at[fs, dn_part(i), grp]
        return remote(rows[b].at[src, grp], dst, dn_zs.at[b, i], dn_zr.at[b, i], {"fs": peer(d)})

    def dn_x(b, i):
        block = dn[b].at[origin(1 + i // 2), dn_part(i), grp]
        return remote(block, block, dn_xs.at[b, i], dn_xr.at[b, i], partner)

    def dn_landed(b, i):
        d = 1 + i // 2
        block = dn[b].at[origin(d), dn_part(i), grp]
        return remote(block, block, dn_zs.at[b, i], dn_zr.at[b, i], {"fs": origin(d)})

    gu_list = [("gu", i) for i in range((n_fs - 1) * base)]
    dn_list = [("dn", i) for i in range((n_fs - 1) * 2)]

    def piece(kind, i):
        if kind == "gu":
            return gu_z, gu_landed, gu_x, gu_cond, 1 + i // base
        return dn_z, dn_landed, dn_x, dn_cond, 1 + i // 2

    def issue(b, pieces):
        for kind, i in pieces:
            along_z, _, _, cond, d = piece(kind, i)
            when(cond(i, peer(d)), lambda: along_z(b, i).start())

    def forward(b, pieces):
        for kind, i in pieces:
            _, landed, along_x, cond, _ = piece(kind, i)

            def go():
                landed(b, i).wait_recv()
                along_x(b, i).start()

            when(cond(i, fs), go)

    def collect(b, pieces):
        for kind, i in pieces:
            _, _, along_x, cond, _ = piece(kind, i)
            when(cond(i, fs), lambda: along_x(b, i).wait_recv())

    def drain(b, pieces):
        for kind, i in pieces:
            along_z, _, along_x, cond, d = piece(kind, i)
            when(cond(i, peer(d)), lambda: along_z(b, i).wait_send())
            when(cond(i, fs), lambda: along_x(b, i).wait_send())

    def load(b, m):
        dst = (wide_gate, wide_up, wide_down)[m]
        return pltpu.make_async_copy(weights[3 * b + m], dst, load_sem.at[m])

    def cast_columns(b):
        load(b, 0).wait()
        load(b, 1).wait()
        half, step = cols[b].shape[2], 32
        for h in range(2):

            def one(r, carry):
                at = pl.ds(pl.multiple_of(h * half + r * step, step), step)
                to = pl.ds(pl.multiple_of(r * step, step), step)
                for t in range(tiles):
                    lane = pl.ds(t * LANES, LANES)
                    cols[b][t, h, to, :LANES] = wide_gate[at, lane].astype(bf)
                    cols[b][t, h, to, LANES:] = wide_up[at, lane].astype(bf)
                return carry

            lax.fori_loop(0, half // step, one, 0)
        own_tiles(cols[b], lambda n: gu[b].at[n, fs])

    def cast_rows(b):
        load(b, 2).wait()
        half = rows[b].shape[2]

        def one(i, carry):
            at = pl.ds(pl.multiple_of(i * half, half), half)
            rows[b][lax.div(i, 2), lax.rem(i, 2)] = wide_down[at, :].astype(bf)
            return carry

        lax.fori_loop(0, 2 * tiles, one, 0)
        own_tiles(rows[b], lambda n: dn[b].at[fs, n])

    def own_tiles(src, dst):
        start = first_tile(fs)
        for n in range(base):
            def copy():
                dst(n)[...] = src[start + n]

            if n < base - 1 or not short:
                copy()
            else:
                pl.when(has_last(fs))(copy)

    def blank_tiles(b):
        if short:
            @pl.when(jnp.logical_not(has_last(fs)))
            def _():
                gu[b][base - 1] = jnp.zeros(gu[b].shape[1:], bf)
                for a in range(n_fs):
                    dn[b][a, base - 1] = jnp.zeros(dn[b].shape[2:], bf)

    def ag_right(b, o):
        block = x[b].at[tp, o]
        return remote(block, block, ag_zs.at[b, 0, o], ag_zr.at[b, o], {"fs": peer(1)})

    def ag_left(b, o):
        block = x[b].at[tp, o]
        return remote(block, block, ag_zs.at[b, 1, o], ag_zr.at[b, o], {"fs": origin(1)})

    def ag_y(b, o, mine=True):
        block = x[b].at[tp if mine else far_tp, o]
        return remote(block, block, ag_ys.at[b, o], ag_yr.at[b, o], across)

    def ag_core(b, o, j):
        block = x[b].at[far_tp if j else tp, o]
        return remote(block, block, ag_cs.at[b, j, o], ag_cr.at[b, j, o], other_core)

    def ag_own(b):
        pl.when(fs < last)(lambda: ag_right(b, fs).start())
        pl.when(fs > 0)(lambda: ag_left(b, fs).start())
        ag_y(b, fs).start()
        ag_core(b, fs, 0).start()

    def ag_hop(b, h):
        @pl.when(fs - 1 - h >= 0)
        def _():
            o = fs - 1 - h
            ag_right(b, o).wait_recv()
            pl.when(fs < last)(lambda: ag_right(b, o).start())
            ag_y(b, o).start()
            ag_core(b, o, 0).start()

        @pl.when(fs + 1 + h <= last)
        def _():
            o = fs + 1 + h
            ag_left(b, o).wait_recv()
            pl.when(fs > 0)(lambda: ag_left(b, o).start())
            ag_y(b, o).start()
            ag_core(b, o, 0).start()

    def ag_share(b, o):
        ag_y(b, o, False).wait_recv()
        ag_core(b, o, 1).start()

    def ag_share_hop(b, h):
        pl.when(fs - 1 - h >= 0)(lambda: ag_share(b, fs - 1 - h))
        pl.when(fs + 1 + h <= last)(lambda: ag_share(b, fs + 1 + h))

    def ag_finish(b):
        for o in range(n_fs):
            for j in range(2):
                ag_core(b, o, j).wait_recv()

    def ag_drain(b):
        for o in range(n_fs):
            if o < last:
                pl.when((fs < last) & (fs >= o))(lambda: ag_right(b, o).wait_send())
            if o > 0:
                pl.when((fs > 0) & (fs <= o))(lambda: ag_left(b, o).wait_send())
            ag_y(b, o).wait_send()
            for j in range(2):
                ag_core(b, o, j).wait_send()

    def norm(b):
        count, step = x[b].shape[2], 64
        width = x[b].shape[3]
        per = count // step

        def one(i, carry):
            k, at = lax.div(i, per), pl.ds(pl.multiple_of(lax.rem(i, per) * step, step), step)
            squares = jnp.zeros((step, width), f32)
            for t in range(n_tp):
                v = x[b][t, k, at, :].astype(f32)
                squares = squares + v * v
            mean = jnp.sum(squares, axis=1, keepdims=True) / (width * n_tp)
            factor = lax.rsqrt(mean + epsilon)
            for t in range(n_tp):
                v = x[b][t, k, at, :].astype(f32) * factor * all_gains[t, b : b + 1, :]
                normed[k, at, t * width : (t + 1) * width] = v.astype(bf)
            return carry

        lax.fori_loop(0, n_fs * per, one, 0)

    def make_hidden(b):
        start = first_tile(fs)

        def one(k, carry):
            for n in range(base):
                part = gu[b][n].reshape(-1, 2 * LANES)
                both = jnp.dot(normed[k], part, preferred_element_type=f32)
                gate = both[:, :LANES] * scales[2 * b, start + n]
                up = both[:, LANES:] * scales[2 * b + 1, start + n]
                value = gate / (1.0 + jnp.exp(-gate)) * up
                hidden[k, :, n * LANES : (n + 1) * LANES] = value.astype(bf)
            return carry

        lax.fori_loop(0, n_fs, one, 0)

    def term(b, a, k):
        part = dn[b][a].reshape(-1, dn[b].shape[4])
        return jnp.dot(hidden[k], part, preferred_element_type=f32)

    def rs_core(b, j, k):
        return remote(core_out.at[j, k], from_core[b].at[j, k], rs_cs.at[b, j, k], rs_cr.at[b, j, k], other_core)

    def rs_y(b, k):
        return remote(y_out.at[k], from_y[b].at[k], rs_ys.at[b, k], rs_yr.at[b, k], across)

    def rs_right(b, k):
        return remote(z_out.at[k], from_left[b].at[k], rs_zs.at[b, k], rs_lr.at[b, k], {"fs": peer(1)})

    def rs_left(b, k):
        return remote(z_out.at[k], from_right[b].at[k], rs_zs.at[b, k], rs_rr.at[b, k], {"fs": origin(1)})

    def turn(kk):
        odd = lax.rem(kk, 2)
        k = (1 - odd) * (last - lax.div(kk, 2)) + odd * lax.div(kk, 2)
        flip = lax.div(2 * fs, n_fs)
        return k + flip * (last - 2 * k)

    def scatter(b, hook):
        for j in range(2):
            target = 2 * (1 - chip if j == 0 else chip) + 1 - core

            def one(kk, carry):
                k = turn(kk)
                core_out[j, k] = term(b, target, k).astype(bf)
                rs_core(b, j, k).start()
                return carry

            lax.fori_loop(0, n_fs, one, 0)
        hook("core")

        def two(kk, carry):
            k = turn(kk)
            value = term(b, far_tp, k)
            rs_core(b, 0, k).wait_recv()
            y_out[k] = (value + from_core[b][0, k].astype(f32)).astype(bf)
            rs_y(b, k).start()
            return carry

        lax.fori_loop(0, n_fs, two, 0)
        hook("y")
        for kk in range(n_fs):
            k = turn(kk)
            rs_core(b, 1, k).wait_recv()
            total[...] = term(b, tp, k) + from_core[b][1, k].astype(f32)
            rs_y(b, k).wait_recv()
            total[...] = total[...] + from_y[b][k].astype(f32)

            @pl.when((k > fs) & (fs > 0))
            def _():
                rs_right(b, k).wait_recv()
                total[...] = total[...] + from_left[b][k].astype(f32)

            @pl.when((k < fs) & (fs < last))
            def _():
                rs_left(b, k).wait_recv()
                total[...] = total[...] + from_right[b][k].astype(f32)

            @pl.when(k == fs)
            def _():
                kept[...] = total[...]

            @pl.when(k != fs)
            def _():
                z_out[k] = total[...].astype(bf)

            pl.when(k > fs)(lambda: rs_right(b, k).start())
            pl.when(k < fs)(lambda: rs_left(b, k).start())
            hook(kk)

        @pl.when(fs > 0)
        def _():
            rs_right(b, fs).wait_recv()
            kept[...] = kept[...] + from_left[b][fs].astype(f32)

        @pl.when(fs < last)
        def _():
            rs_left(b, fs).wait_recv()
            kept[...] = kept[...] + from_right[b][fs].astype(f32)

        value = x[b][tp, fs].astype(f32) + 0.5 * kept[...] * down_scales[b : b + 1, :]
        return value.astype(bf)

    def scatter_drain(b):
        for k in range(n_fs):
            for j in range(2):
                rs_core(b, j, k).wait_send()
            rs_y(b, k).wait_send()
            pl.when(fs < k)(lambda: rs_right(b, k).wait_send())
            pl.when(fs > k)(lambda: rs_left(b, k).wait_send())

    own_tokens = pltpu.make_async_copy(tokens, x[0].at[tp, fs], load_sem.at[3])
    own_tokens.start()
    for m in range(3):
        load(0, m).start()

    barrier = pltpu.get_barrier_semaphore()
    greeted = [{"fs": peer(d)} for d in range(1, n_fs)] + [partner]
    greeted = greeted + [{"tp": lax.rem(tp + r, n_tp)} for r in range(1, n_tp)]
    for device in greeted:
        pl.semaphore_signal(barrier, inc=1, device_id=device, device_id_type=MESH)
    pl.semaphore_wait(barrier, len(greeted))

    def gain_copy(r):
        return remote(
            gains, all_gains.at[tp], gain_send.at[r - 1], gain_recv.at[r - 1], {"tp": lax.rem(tp + r, n_tp)}
        )

    own_tokens.wait()
    ag_own(0)
    for r in range(1, n_tp):
        gain_copy(r).start()
    all_gains[tp] = gains[...]
    for b in range(2):
        blank_tiles(b)
    cast_columns(0)
    load(1, 0).start()
    load(1, 1).start()
    issue(0, gu_list[:2])
    ag_hop(0, 0)
    issue(0, gu_list[2:4])
    ag_share(0, fs)
    ag_hop(0, 1)
    issue(0, gu_list[4:6])
    ag_share_hop(0, 0)
    for h in range(2, last):
        ag_hop(0, h)
    issue(0, gu_list[6:])
    cast_rows(0)
    load(1, 2).start()
    issue(0, dn_list)
    cut = len(gu_list) // 3
    forward(0, gu_list[:cut])
    for h in range(1, last):
        ag_share_hop(0, h)
    cast_columns(1)
    forward(0, gu_list[cut : 2 * cut])
    cast_rows(1)
    ag_finish(0)
    for r in range(1, n_tp):
        gain_copy(r).wait_recv()
    norm(0)
    forward(0, gu_list[2 * cut :])
    collect(0, gu_list)
    make_hidden(0)
    every = gu_list + dn_list
    issue(1, every[:5])
    forward(0, dn_list)
    collect(0, dn_list)

    def hook(stage):
        if stage == 0:
            forward(1, every[0:2])
            issue(1, every[5:7])
        if stage == 1:
            forward(1, every[2:4])
            issue(1, every[7:8])
        if stage == 2:
            forward(1, every[4:6])
            issue(1, every[8:9])
        if stage == 3:
            issue(1, every[9:10])

    x[1][tp, fs] = scatter(0, hook)
    ag_own(1)
    issue(1, every[10:11])
    forward(1, every[6:8])
    ag_hop(1, 0)
    issue(1, every[11:12])
    ag_share(1, fs)
    forward(1, every[8:9])
    ag_hop(1, 1)
    issue(1, every[12:13])
    ag_share_hop(1, 0)
    forward(1, every[9:10])
    for h in range(2, last):
        ag_hop(1, h)
    issue(1, every[13:])
    for h in range(1, last):
        ag_share_hop(1, h)
        forward(1, every[9 + h : 10 + h])
    forward(1, every[9 + last :])
    scatter_drain(0)
    ag_finish(1)
    norm(1)
    collect(1, gu_list)
    make_hidden(1)
    collect(1, dn_list)
    out[...] = scatter(1, lambda stage: None)
    scatter_drain(1)
    for b in range(2):
        ag_drain(b)
        drain(b, every)
    for r in range(1, n_tp):
        gain_copy(r).wait_send()


def body_kernel(tokens, *rest):
    first, second = rest[:7], rest[7:]
    n_fs, n_tp = lax.axis_size("fs"), lax.axis_size("tp")
    count, feats = tokens.shape
    depth, units = first[1].shape
    tiles = units // LANES
    base = -(-tiles // n_fs)
    half = depth // 2
    bf, f32 = jnp.bfloat16, jnp.float32
    gains = jnp.stack([first[0], second[0]])
    scales = jnp.stack([first[2], first[4], second[2], second[4]]).reshape(4, tiles, 1, LANES)
    scales = jnp.pad(scales, ((0, 0), (0, base), (0, 0), (0, 0)))
    down_scales = jnp.stack([first[6], second[6]])
    weights = [first[1], first[3], first[5], second[1], second[3], second[5]]
    vmem, dma = pltpu.VMEM, pltpu.SemaphoreType.DMA
    any_spec, vmem_spec = pl.BlockSpec(memory_space=pl.ANY), pl.BlockSpec(memory_space=pltpu.VMEM)
    tile = (count, feats)
    scratch = [
        vmem((depth, units), f32), vmem((depth, units), f32), vmem((units, feats), f32),
        vmem((n_tp, 2, feats), f32),
    ]
    scratch += [vmem((tiles, 2, half, 2 * LANES), bf)] * 2
    scratch += [vmem((tiles, 2, LANES // 2, feats), bf)] * 2
    scratch += [vmem((base, n_fs, 2, half, 2 * LANES), bf)] * 2
    scratch += [vmem((n_fs, base, 2, LANES // 2, feats), bf)] * 2
    scratch += [vmem((n_tp, n_fs, *tile), bf)] * 2
    scratch += [vmem((n_fs, count, n_tp * feats), bf), vmem((n_fs, count, base * LANES), bf)]
    scratch += [vmem((2, n_fs, *tile), bf)] * 3
    scratch += [vmem((n_fs, *tile), bf)] * 3
    scratch += [vmem((n_fs, *tile), bf)] * 5
    scratch += [vmem(tile, f32)] * 2
    scratch += [dma((4,)), dma((n_tp - 1,)), dma((n_tp - 1,))]
    scratch += [dma((2, 2, n_fs)), dma((2, n_fs)), dma((2, n_fs)), dma((2, n_fs)), dma((2, 2, n_fs)), dma((2, 2, n_fs))]
    scratch += [dma((2, (n_fs - 1) * base))] * 4 + [dma((2, (n_fs - 1) * 2))] * 4
    scratch += [dma((2, 2, n_fs))] * 2 + [dma((2, n_fs))] * 5
    return pl.pallas_call(
        functools.partial(both_blocks, n_fs, n_tp, tiles),
        out_shape=jax.ShapeDtypeStruct(tile, bf),
        in_specs=[any_spec] + [vmem_spec] * 3 + [any_spec] * 6,
        out_specs=vmem_spec,
        scratch_shapes=scratch,
        compiler_params=pltpu.CompilerParams(
            collective_id=0, has_side_effects=True, vmem_limit_bytes=67043328
        ),
    )(tokens, gains, scales, down_scales, *weights)


def fits(tokens, *rest):
    n_grp, n_fs, n_tp = (lax.axis_size(name) for name in ("grp", "fs", "tp"))
    depth, units = rest[1].shape
    return (
        n_grp == 2
        and n_fs == n_tp
        and n_tp == 4
        and units % LANES == 0
        and units // LANES > n_fs
        and depth % 64 == 0
        and depth == tokens.shape[1]
        and depth % LANES == 0
        and tokens.shape[0] % 64 == 0
    )


def solution(mesh):
    in_specs = (
        P(("grp", "fs"), "tp"),
        P("tp"),
        P("fs", "tp"),
        P("tp"),
        P("fs", "tp"),
        P("tp"),
        P("tp", "fs"),
        P("tp"),
        P("tp"),
        P("fs", "tp"),
        P("tp"),
        P("fs", "tp"),
        P("tp"),
        P("tp", "fs"),
        P("tp"),
    )
    out_specs = P(("grp", "fs"), "tp")

    def body(*args):
        return (body_kernel if fits(*args) else body_gather)(*args)

    return jax.shard_map(body, mesh=mesh, in_specs=in_specs, out_specs=out_specs, check_vma=False)
```

```python
import functools

import jax
import jax.numpy as jnp
from jax import lax
from jax.experimental import pallas as pl
from jax.experimental.pallas import tpu as pltpu
from jax.sharding import PartitionSpec as P

MESH = pl.DeviceIdType.MESH
LANES = 128
PARTS = 2

epsilon = 1e-06


def normalize(stream, gain):
    values = stream.astype(jnp.float32)
    totals = lax.psum(jnp.sum(values * values, axis=1), "tp")
    width = values.shape[1] * lax.axis_size("tp")
    normed = (values * lax.rsqrt(totals / width + epsilon)[:, None] * gain).astype(jnp.bfloat16)
    return values, lax.all_gather(normed, "tp", axis=1, tiled=True)


def gathered_block(stream, gain, gate_w, gate_s, up_w, up_s, down_w, down_s):
    values, whole = normalize(stream, gain)

    def project(weight, scale):
        rows = lax.all_gather(weight.astype(jnp.bfloat16), "fs", axis=0, tiled=True)
        return jnp.dot(whole, rows, preferred_element_type=jnp.float32) * scale

    hidden = (jax.nn.silu(project(gate_w, gate_s)) * project(up_w, up_s)).astype(jnp.bfloat16)
    columns = lax.all_gather(down_w.astype(jnp.bfloat16), "fs", axis=1, tiled=True)
    terms = jnp.dot(hidden, columns, preferred_element_type=jnp.float32).astype(jnp.bfloat16)
    summed = lax.psum_scatter(terms, "tp", scatter_dimension=1, tiled=True).astype(jnp.float32)
    return (values + 0.5 * summed * down_s).astype(jnp.bfloat16)


def body_gather(tokens, *rest):
    middle = gathered_block(tokens, *rest[:7])
    return gathered_block(middle, *rest[7:])


def both_blocks(n_fs, n_tp, tiles, parts, *refs):
    tokens, small, weights, out, refs = refs[0], refs[1:9], refs[9:15], refs[15], refs[16:]
    (
        wide_gate, wide_up, wide_down, gains, all_gains, scales, down_scales,
        cols_0, cols_1, rows_0, rows_1, gu_0, gu_1, dn_0, dn_1, x_0, x_1, normed, hidden,
        core_out, from_core_0, from_core_1, y_out, from_y_0, from_y_1,
        z_out, from_left_0, from_left_1, from_right_0, from_right_1, total, kept,
        load_sem, small_sem, gain_send, gain_recv,
        ag_zs, ag_zr, ag_ys, ag_yr, ag_cs, ag_cr,
        gu_zs, gu_zr, gu_xs, gu_xr, dn_zs, dn_zr, dn_xs, dn_xr,
        rs_cs, rs_cr, rs_ys, rs_yr, rs_zs, rs_lr, rs_rr,
    ) = refs
    cols, rows, gu, dn, x = (cols_0, cols_1), (rows_0, rows_1), (gu_0, gu_1), (dn_0, dn_1), (x_0, x_1)
    from_core, from_y = (from_core_0, from_core_1), (from_y_0, from_y_1)
    from_left, from_right = (from_left_0, from_left_1), (from_right_0, from_right_1)

    grp, fs, tp = lax.axis_index("grp"), lax.axis_index("fs"), lax.axis_index("tp")
    core, chip = lax.rem(tp, 2), lax.div(tp, 2)
    partner, other_core, across = {"grp": 1 - grp}, {"tp": tp + 1 - 2 * core}, {"tp": lax.rem(tp + 2, n_tp)}
    far_tp = lax.rem(tp + 2, n_tp)
    last = n_fs - 1
    base = -(-tiles // n_fs)
    short = n_fs * base - tiles
    bf, f32 = jnp.bfloat16, jnp.float32

    def first_tile(dev):
        even = jnp.minimum(dev, short)
        odd = jnp.maximum(dev - (n_fs - short), 0)
        return dev * base - (1 - core) * even - core * odd

    def has_last(dev):
        return first_tile(dev + 1) - first_tile(dev) == base

    def peer(d):
        return lax.rem(fs + d, n_fs)

    def other(j):
        flip = lax.div(2 * fs, n_fs)
        place = fs + flip * (last - 2 * fs)
        o = j + jnp.where(place <= j, 1, 0)
        return o + flip * (last - 2 * o)

    def remote(src, dst, sends, recvs, device):
        return pltpu.make_async_remote_copy(
            src_ref=src, dst_ref=dst, send_sem=sends, recv_sem=recvs, device_id=device, device_id_type=MESH
        )

    def when(cond, fn):
        if cond is None:
            fn()
        else:
            pl.when(cond)(fn)

    def gu_cond(i, dev):
        return has_last(dev) if i // last == base - 1 and short else None

    def gu_z(b, i):
        to, n = other(i % last), i // last
        src = cols[b].at[first_tile(to) + n, grp]
        return remote(src, gu[b].at[n, fs, grp], gu_zs.at[b, i], gu_zr.at[b, n, fs], {"fs": to})

    def gu_landed(b, i):
        o, n = other(i % last), i // last
        block = gu[b].at[n, o, grp]
        return remote(block, block, gu_zs.at[b, i], gu_zr.at[b, n, o], {"fs": o})

    def gu_x(b, i):
        block = gu[b].at[i // last, other(i % last), grp]
        return remote(block, block, gu_xs.at[b, i], gu_xr.at[b, i], partner)

    def dn_part(i):
        return pl.ds(0, base - 1) if i < last else pl.ds(base - 1, 1)

    def dn_cond(i, dev):
        return has_last(dev) if i >= last and short else None

    def dn_z(b, i):
        to = other(i % last)
        start = first_tile(to)
        src = pl.ds(start, base - 1) if i < last else pl.ds(start + base - 1, 1)
        dst = dn[b].at[fs, dn_part(i), grp]
        return remote(rows[b].at[src, grp], dst, dn_zs.at[b, i], dn_zr.at[b, i // last, fs], {"fs": to})

    def dn_landed(b, i):
        o = other(i % last)
        block = dn[b].at[o, dn_part(i), grp]
        return remote(block, block, dn_zs.at[b, i], dn_zr.at[b, i // last, o], {"fs": o})

    def dn_x(b, i):
        block = dn[b].at[other(i % last), dn_part(i), grp]
        return remote(block, block, dn_xs.at[b, i], dn_xr.at[b, i], partner)

    gu_list = [("gu", i) for i in range((n_fs - 1) * base)]
    dn_list = [("dn", i) for i in range((n_fs - 1) * 2)]

    def piece(kind, i):
        if kind == "gu":
            return gu_z, gu_landed, gu_x, gu_cond, i % last
        return dn_z, dn_landed, dn_x, dn_cond, i % last

    def issue(b, pieces):
        for kind, i in pieces:
            along_z, _, _, cond, j = piece(kind, i)
            when(cond(i, other(j)), lambda: along_z(b, i).start())

    def forward(b, pieces):
        for kind, i in pieces:
            _, landed, along_x, cond, _ = piece(kind, i)

            def go():
                landed(b, i).wait_recv()
                along_x(b, i).start()

            when(cond(i, fs), go)

    def collect(b, pieces):
        for kind, i in pieces:
            _, _, along_x, cond, _ = piece(kind, i)
            when(cond(i, fs), lambda: along_x(b, i).wait_recv())

    def drain(b, pieces):
        for kind, i in pieces:
            along_z, _, along_x, cond, j = piece(kind, i)
            when(cond(i, other(j)), lambda: along_z(b, i).wait_send())
            when(cond(i, fs), lambda: along_x(b, i).wait_send())

    def load(b, m):
        dst = (wide_gate, wide_up, wide_down)[m]
        return pltpu.make_async_copy(weights[3 * b + m], dst, load_sem.at[m])

    def cast_columns(b):
        load(b, 0).wait()
        load(b, 1).wait()
        half, step = cols[b].shape[2], 32
        for h in range(2):

            def one(r, carry):
                at = pl.ds(pl.multiple_of(h * half + r * step, step), step)
                to = pl.ds(pl.multiple_of(r * step, step), step)
                for t in range(tiles):
                    lane = pl.ds(t * LANES, LANES)
                    cols[b][t, h, to, :LANES] = wide_gate[at, lane].astype(bf)
                    cols[b][t, h, to, LANES:] = wide_up[at, lane].astype(bf)
                return carry

            lax.fori_loop(0, half // step, one, 0)
        own_tiles(cols[b], lambda n: gu[b].at[n, fs])

    def cast_rows(b):
        load(b, 2).wait()
        half = rows[b].shape[2]

        def one(i, carry):
            at = pl.ds(pl.multiple_of(i * half, half), half)
            rows[b][lax.div(i, 2), lax.rem(i, 2)] = wide_down[at, :].astype(bf)
            return carry

        lax.fori_loop(0, 2 * tiles, one, 0)
        own_tiles(rows[b], lambda n: dn[b].at[fs, n])

    def own_tiles(src, dst):
        start = first_tile(fs)
        for n in range(base):
            def copy():
                dst(n)[...] = src[start + n]

            if n < base - 1 or not short:
                copy()
            else:
                pl.when(has_last(fs))(copy)

    def blank_tiles(b):
        if short:
            @pl.when(jnp.logical_not(has_last(fs)))
            def _():
                gu[b][base - 1] = jnp.zeros(gu[b].shape[1:], bf)
                for a in range(n_fs):
                    dn[b][a, base - 1] = jnp.zeros(dn[b].shape[2:], bf)

    def part(q):
        rows_q = x[0].shape[2] // parts
        return pl.ds(q * rows_q, rows_q)

    def ag_right(b, o, q):
        block = x[b].at[tp, o, part(q)]
        return remote(block, block, ag_zs.at[b, 0, o, q], ag_zr.at[b, o, q], {"fs": peer(1)})

    def ag_left(b, o, q):
        block = x[b].at[tp, o, part(q)]
        return remote(block, block, ag_zs.at[b, 1, o, q], ag_zr.at[b, o, q], {"fs": peer(last)})

    def ag_y(b, o, q, mine=True):
        block = x[b].at[tp if mine else far_tp, o, part(q)]
        return remote(block, block, ag_ys.at[b, o, q], ag_yr.at[b, o, q], across)

    def ag_core(b, o, q, j):
        block = x[b].at[far_tp if j else tp, o, part(q)]
        return remote(block, block, ag_cs.at[b, j, o, q], ag_cr.at[b, j, o, q], other_core)

    def ag_own(b, q):
        pl.when(fs < last)(lambda: ag_right(b, fs, q).start())
        pl.when(fs > 0)(lambda: ag_left(b, fs, q).start())
        ag_y(b, fs, q).start()
        ag_core(b, fs, q, 0).start()

    def ag_hop(b, h):
        for q in range(parts):
            @pl.when(fs - 1 - h >= 0)
            def _():
                o = fs - 1 - h
                ag_right(b, o, q).wait_recv()
                pl.when(fs < last)(lambda: ag_right(b, o, q).start())
                ag_y(b, o, q).start()
                ag_core(b, o, q, 0).start()

            @pl.when(fs + 1 + h <= last)
            def _():
                o = fs + 1 + h
                ag_left(b, o, q).wait_recv()
                pl.when(fs > 0)(lambda: ag_left(b, o, q).start())
                ag_y(b, o, q).start()
                ag_core(b, o, q, 0).start()

    def ag_share(b, o):
        for q in range(parts):
            ag_y(b, o, q, False).wait_recv()
            ag_core(b, o, q, 1).start()

    def ag_share_hop(b, h):
        pl.when(fs - 1 - h >= 0)(lambda: ag_share(b, fs - 1 - h))
        pl.when(fs + 1 + h <= last)(lambda: ag_share(b, fs + 1 + h))

    def ag_arrived(b, o):
        for q in range(parts):
            for j in range(2):
                ag_core(b, o, q, j).wait_recv()

    def ag_drain(b):
        for o in range(n_fs):
            for q in range(parts):
                if o < last:
                    pl.when((fs < last) & (fs >= o))(lambda: ag_right(b, o, q).wait_send())
                if o > 0:
                    pl.when((fs > 0) & (fs <= o))(lambda: ag_left(b, o, q).wait_send())
                ag_y(b, o, q).wait_send()
                for j in range(2):
                    ag_core(b, o, q, j).wait_send()

    def norm(b, k):
        step, width = 64, x[b].shape[3]

        def one(i, carry):
            at = pl.ds(pl.multiple_of(i * step, step), step)
            squares = jnp.zeros((step, width), f32)
            for t in range(n_tp):
                v = x[b][t, k, at, :].astype(f32)
                squares = squares + v * v
            mean = jnp.sum(squares, axis=1, keepdims=True) / (width * n_tp)
            factor = lax.rsqrt(mean + epsilon)
            for t in range(n_tp):
                v = x[b][t, k, at, :].astype(f32) * factor * all_gains[t, b]
                normed[k, at, t * width : (t + 1) * width] = v.astype(bf)
            return carry

        lax.fori_loop(0, x[b].shape[2] // step, one, 0)

    def make_hidden(b, k):
        for n in range(base):
            weight = gu[b][n].reshape(-1, 2 * LANES)
            both = jnp.dot(normed[k], weight, preferred_element_type=f32)
            gate = both[:, :LANES] * scales[2 * b, n]
            up = both[:, LANES:] * scales[2 * b + 1, n]
            value = gate / (1.0 + jnp.exp(-gate)) * up
            hidden[k, :, n * LANES : (n + 1) * LANES] = value.astype(bf)

    def every_block(fn):
        def one(k, carry):
            fn(k)
            return carry

        lax.fori_loop(0, n_fs, one, 0)

    def both_sides(h, fn):
        def one(side, carry):
            k = fs + (2 * side - 1) * (1 + h)
            pl.when((k >= 0) & (k <= last))(lambda: fn(k))
            return carry

        lax.fori_loop(0, 2, one, 0)

    def term(b, a, k):
        weight = dn[b][a].reshape(-1, dn[b].shape[4])
        return jnp.dot(hidden[k], weight, preferred_element_type=f32)

    def rs_core(b, j, k, q):
        src, dst = core_out.at[j, k, part(q)], from_core[b].at[j, k, part(q)]
        return remote(src, dst, rs_cs.at[b, j, k, q], rs_cr.at[b, j, k, q], other_core)

    def rs_y(b, k, q):
        src, dst = y_out.at[k, part(q)], from_y[b].at[k, part(q)]
        return remote(src, dst, rs_ys.at[b, k, q], rs_yr.at[b, k, q], across)

    def rs_right(b, k, q):
        src, dst = z_out.at[k, part(q)], from_left[b].at[k, part(q)]
        return remote(src, dst, rs_zs.at[b, k, q], rs_lr.at[b, k, q], {"fs": peer(1)})

    def rs_left(b, k, q):
        src, dst = z_out.at[k, part(q)], from_right[b].at[k, part(q)]
        return remote(src, dst, rs_zs.at[b, k, q], rs_rr.at[b, k, q], {"fs": peer(last)})

    def turn(kk):
        odd = lax.rem(kk, 2)
        k = (1 - odd) * (last - lax.div(kk, 2)) + odd * lax.div(kk, 2)
        flip = lax.div(2 * fs, n_fs)
        return k + flip * (last - 2 * k)

    def scatter(b, hook, finish):
        def to_core(j):
            target = 2 * (1 - chip if j == 0 else chip) + 1 - core

            def one(kk, carry):
                k = turn(kk)
                core_out[j, k] = term(b, target, k).astype(bf)
                for q in range(parts):
                    rs_core(b, j, k, q).start()
                return carry

            lax.fori_loop(0, n_fs, one, 0)

        def to_y(kk, carry):
            k = turn(kk)
            total[...] = term(b, far_tp, k)
            for q in range(parts):
                rs_core(b, 0, k, q).wait_recv()
                y_out[k, part(q)] = (total[part(q)] + from_core[b][0, k, part(q)].astype(f32)).astype(bf)
                rs_y(b, k, q).start()
            return carry

        to_core(0)
        hook("core")
        lax.fori_loop(0, n_fs, to_y, 0)
        to_core(1)
        hook("y")
        for kk in range(n_fs):
            k = turn(kk)
            total[...] = term(b, tp, k)
            for q in range(parts):
                at = part(q)
                rs_core(b, 1, k, q).wait_recv()
                rs_y(b, k, q).wait_recv()
                total[at] = total[at] + from_core[b][1, k, at].astype(f32) + from_y[b][k, at].astype(f32)

                @pl.when((k > fs) & (fs > 0))
                def _():
                    rs_right(b, k, q).wait_recv()
                    total[at] = total[at] + from_left[b][k, at].astype(f32)

                @pl.when((k < fs) & (fs < last))
                def _():
                    rs_left(b, k, q).wait_recv()
                    total[at] = total[at] + from_right[b][k, at].astype(f32)

                @pl.when(k == fs)
                def _():
                    kept[at] = total[at]

                @pl.when(k != fs)
                def _():
                    z_out[k, at] = total[at].astype(bf)

                pl.when(k > fs)(lambda: rs_right(b, k, q).start())
                pl.when(k < fs)(lambda: rs_left(b, k, q).start())
            hook(kk)

        for q in range(parts):
            at = part(q)

            @pl.when(fs > 0)
            def _():
                rs_right(b, fs, q).wait_recv()
                kept[at] = kept[at] + from_left[b][fs, at].astype(f32)

            @pl.when(fs < last)
            def _():
                rs_left(b, fs, q).wait_recv()
                kept[at] = kept[at] + from_right[b][fs, at].astype(f32)

            value = x[b][tp, fs, at].astype(f32) + 0.5 * kept[at] * down_scales[b]
            finish(q, value.astype(bf))

    def scatter_drain(b):
        for k in range(n_fs):
            for q in range(parts):
                for j in range(2):
                    rs_core(b, j, k, q).wait_send()
                rs_y(b, k, q).wait_send()
                pl.when(fs < k)(lambda: rs_right(b, k, q).wait_send())
                pl.when(fs > k)(lambda: rs_left(b, k, q).wait_send())

    own_tokens = pltpu.make_async_copy(tokens, x[0].at[tp, fs], load_sem.at[3])
    own_tokens.start()
    small_loads = []

    def small_load(src, dst):
        small_loads.append(pltpu.make_async_copy(src, dst, small_sem.at[len(small_loads)]))

    for b in range(2):
        gain, gate_s, up_s, down_s = small[4 * b : 4 * b + 4]
        small_load(gain, gains.at[b])
        small_load(down_s, down_scales.at[b])
        for n in range(base):
            at = pl.multiple_of(jnp.minimum(first_tile(fs) + n, tiles - 1) * LANES, LANES)
            for i, src in enumerate((gate_s, up_s)):
                small_load(src.at[:, pl.ds(at, LANES)], scales.at[2 * b + i, n])
    for copy in small_loads:
        copy.start()
    for m in range(3):
        load(0, m).start()

    barrier = pltpu.get_barrier_semaphore()
    greeted = [{"fs": peer(d)} for d in range(1, n_fs)] + [partner]
    greeted = greeted + [{"tp": lax.rem(tp + r, n_tp)} for r in range(1, n_tp)]
    for device in greeted:
        pl.semaphore_signal(barrier, inc=1, device_id=device, device_id_type=MESH)
    pl.semaphore_wait(barrier, len(greeted))

    def gain_copy(r):
        return remote(
            gains, all_gains.at[tp], gain_send.at[r - 1], gain_recv.at[r - 1], {"tp": lax.rem(tp + r, n_tp)}
        )

    own_tokens.wait()
    for q in range(parts):
        ag_own(0, q)
    for copy in small_loads:
        copy.wait()
    for r in range(1, n_tp):
        gain_copy(r).start()
    all_gains[tp] = gains[...]
    for b in range(2):
        blank_tiles(b)
    every = gu_list + dn_list
    count = len(gu_list)
    cast_columns(0)
    issue(0, every[:1])
    cast_rows(0)
    for m in range(3):
        load(1, m).start()
    ag_hop(0, 0)
    issue(0, every[1 : 2 * last])
    ag_share(0, fs)
    cast_columns(1)
    ag_hop(0, 1)
    issue(0, every[2 * last :])
    forward(0, every[:last])
    ag_share_hop(0, 0)
    cast_rows(1)
    forward(0, every[last : 2 * last])
    for h in range(2, last):
        ag_hop(0, h)
    ag_share_hop(0, 1)
    forward(0, every[2 * last : 3 * last - 1])
    for h in range(2, last):
        ag_share_hop(0, h)
    forward(0, every[3 * last - 1 : count])
    issue(1, every[:6])
    for r in range(1, n_tp):
        gain_copy(r).wait_recv()
    for o in range(n_fs):
        ag_arrived(0, o)
    every_block(lambda k: norm(0, k))
    forward(0, every[count : count + 2])
    collect(0, every[:count])
    every_block(lambda k: make_hidden(0, k))
    forward(0, every[count + 2 :])
    collect(0, every[count:])

    def hook(stage):
        if stage == "core":
            issue(1, every[6:8])
        if stage == 0:
            issue(1, every[8:9])
            forward(1, every[0:2])
        if stage == 1:
            issue(1, every[9:10])
            forward(1, every[2:3])
        if stage == 2:
            issue(1, every[10:11])
            forward(1, every[3:4])
        if stage == 3:
            forward(1, every[4:6])

    def pass_on(q, value):
        x[1][tp, fs, part(q)] = value
        ag_own(1, q)

    scatter(0, hook, pass_on)
    forward(1, every[6:7])
    ag_hop(1, 0)
    issue(1, every[11:13])
    ag_share(1, fs)
    forward(1, every[7:8])
    ag_hop(1, 1)
    issue(1, every[13:])
    ag_share_hop(1, 0)
    forward(1, every[8:9])
    ag_arrived(1, fs)
    norm(1, fs)
    for h in range(2, last):
        ag_hop(1, h)
    forward(1, every[9:10])

    def ready(k):
        ag_arrived(1, k)
        norm(1, k)

    for h in range(1, last):
        ag_share_hop(1, h)
        forward(1, every[9 + h : 10 + h])
        both_sides(h - 1, ready)
    forward(1, every[9 + last :])
    both_sides(last - 1, ready)
    collect(1, every[:count])
    every_block(lambda k: make_hidden(1, k))
    scatter_drain(0)
    collect(1, every[count:])

    def put_out(q, value):
        out[part(q)] = value

    scatter(1, lambda stage: None, put_out)
    scatter_drain(1)
    for b in range(2):
        ag_drain(b)
        drain(b, every)
    for r in range(1, n_tp):
        gain_copy(r).wait_send()


def body_kernel(tokens, *rest):
    first, second = rest[:7], rest[7:]
    n_fs, n_tp = lax.axis_size("fs"), lax.axis_size("tp")
    count, feats = tokens.shape
    depth, units = first[1].shape
    tiles = units // LANES
    base = -(-tiles // n_fs)
    half = depth // 2
    bf, f32 = jnp.bfloat16, jnp.float32
    small = []
    for gain, _, gate_s, _, up_s, _, down_s in (first, second):
        small += [gain[None, :], gate_s[None, :], up_s[None, :], down_s[None, :]]
    weights = [first[1], first[3], first[5], second[1], second[3], second[5]]
    vmem, dma = pltpu.VMEM, pltpu.SemaphoreType.DMA
    any_spec, vmem_spec = pl.BlockSpec(memory_space=pl.ANY), pl.BlockSpec(memory_space=pltpu.VMEM)
    tile = (count, feats)
    scratch = [
        vmem((depth, units), f32), vmem((depth, units), f32), vmem((units, feats), f32),
        vmem((2, 1, feats), f32), vmem((n_tp, 2, 1, feats), f32), vmem((4, base, 1, LANES), f32), vmem((2, 1, feats), f32),
    ]
    scratch += [vmem((tiles, 2, half, 2 * LANES), bf)] * 2
    scratch += [vmem((tiles, 2, LANES // 2, feats), bf)] * 2
    scratch += [vmem((base, n_fs, 2, half, 2 * LANES), bf)] * 2
    scratch += [vmem((n_fs, base, 2, LANES // 2, feats), bf)] * 2
    scratch += [vmem((n_tp, n_fs, *tile), bf)] * 2
    scratch += [vmem((n_fs, count, n_tp * feats), bf), vmem((n_fs, count, base * LANES), bf)]
    scratch += [vmem((2, n_fs, *tile), bf)] * 3
    scratch += [vmem((n_fs, *tile), bf)] * 3
    scratch += [vmem((n_fs, *tile), bf)] * 5
    scratch += [vmem(tile, f32)] * 2
    scratch += [dma((4,)), dma((4 + 4 * base,)), dma((n_tp - 1,)), dma((n_tp - 1,))]
    one, two = dma((2, n_fs, PARTS)), dma((2, 2, n_fs, PARTS))
    scratch += [two, one, one, one, two, two]
    for count_of in (base, 2):
        sent = dma((2, (n_fs - 1) * count_of))
        scratch += [sent, dma((2, count_of, n_fs)), sent, sent]
    scratch += [two] * 2 + [one] * 5
    return pl.pallas_call(
        functools.partial(both_blocks, n_fs, n_tp, tiles, PARTS),
        out_shape=jax.ShapeDtypeStruct(tile, bf),
        in_specs=[any_spec] * 15,
        out_specs=vmem_spec,
        scratch_shapes=scratch,
        compiler_params=pltpu.CompilerParams(
            collective_id=0, has_side_effects=True, vmem_limit_bytes=67043328
        ),
    )(tokens, *small, *weights)


def fits(tokens, *rest):
    n_grp, n_fs, n_tp = (lax.axis_size(name) for name in ("grp", "fs", "tp"))
    depth, units = rest[1].shape
    return (
        n_grp == 2
        and n_fs == n_tp
        and n_tp == 4
        and units % LANES == 0
        and units // LANES > n_fs
        and depth % 64 == 0
        and depth == tokens.shape[1]
        and depth % LANES == 0
        and tokens.shape[0] % 64 == 0
    )


def solution(mesh):
    in_specs = (
        P(("grp", "fs"), "tp"),
        P("tp"),
        P("fs", "tp"),
        P("tp"),
        P("fs", "tp"),
        P("tp"),
        P("tp", "fs"),
        P("tp"),
        P("tp"),
        P("fs", "tp"),
        P("tp"),
        P("fs", "tp"),
        P("tp"),
        P("tp", "fs"),
        P("tp"),
    )
    out_specs = P(("grp", "fs"), "tp")

    def body(*args):
        return (body_kernel if fits(*args) else body_gather)(*args)

    return jax.shard_map(body, mesh=mesh, in_specs=in_specs, out_specs=out_specs, check_vma=False)
```

```python
import functools

import jax
import jax.numpy as jnp
from jax import lax
from jax.experimental import pallas as pl
from jax.experimental.pallas import tpu as pltpu
from jax.sharding import PartitionSpec as P

MESH = pl.DeviceIdType.MESH
LANES = 128
PARTS = 2
FIRST = 7
PLAN = {
    "core": (10, 0),
    0: (11, 3),
    1: (12, 5),
    2: (13, 7),
    3: (13, 9),
    "own": (13, 10),
    "hop0": (15, 12),
    "hop1": (15, 13),
    "hop2": (15, 15),
}

epsilon = 1e-06


def normalize(stream, gain):
    values = stream.astype(jnp.float32)
    totals = lax.psum(jnp.sum(values * values, axis=1), "tp")
    width = values.shape[1] * lax.axis_size("tp")
    normed = (values * lax.rsqrt(totals / width + epsilon)[:, None] * gain).astype(jnp.bfloat16)
    return values, lax.all_gather(normed, "tp", axis=1, tiled=True)


def gathered_block(stream, gain, gate_w, gate_s, up_w, up_s, down_w, down_s):
    values, whole = normalize(stream, gain)

    def project(weight, scale):
        rows = lax.all_gather(weight.astype(jnp.bfloat16), "fs", axis=0, tiled=True)
        return jnp.dot(whole, rows, preferred_element_type=jnp.float32) * scale

    hidden = (jax.nn.silu(project(gate_w, gate_s)) * project(up_w, up_s)).astype(jnp.bfloat16)
    columns = lax.all_gather(down_w.astype(jnp.bfloat16), "fs", axis=1, tiled=True)
    terms = jnp.dot(hidden, columns, preferred_element_type=jnp.float32).astype(jnp.bfloat16)
    summed = lax.psum_scatter(terms, "tp", scatter_dimension=1, tiled=True).astype(jnp.float32)
    return (values + 0.5 * summed * down_s).astype(jnp.bfloat16)


def body_gather(tokens, *rest):
    middle = gathered_block(tokens, *rest[:7])
    return gathered_block(middle, *rest[7:])


def both_blocks(n_fs, n_tp, tiles, parts, *refs):
    tokens, small, weights, out, refs = refs[0], refs[1:9], refs[9:15], refs[15], refs[16:]
    (
        wide_gate, wide_up, wide_down, gains, all_gains, scale_0, scale_1, scale_2, scale_3, down_scales,
        cols_0, cols_1, rows_0, rows_1, gu_0, gu_1, dn_0, dn_1, x_0, x_1, normed, hidden,
        core_out, from_core_0, from_core_1, y_out, from_y_0, from_y_1,
        z_out, from_left_0, from_left_1, from_right_0, from_right_1, total, kept,
        load_sem, small_sem, gain_send, gain_recv,
        ag_zs, ag_zr, ag_ys, ag_yr, ag_cs, ag_cr,
        gu_zs, gu_zr, gu_xs, gu_xr, dn_zs, dn_zr, dn_xs, dn_xr,
        rs_cs, rs_cr, rs_ys, rs_yr, rs_zs, rs_lr, rs_rr,
    ) = refs
    scales = (scale_0, scale_1, scale_2, scale_3)
    cols, rows, gu, dn, x = (cols_0, cols_1), (rows_0, rows_1), (gu_0, gu_1), (dn_0, dn_1), (x_0, x_1)
    from_core, from_y = (from_core_0, from_core_1), (from_y_0, from_y_1)
    from_left, from_right = (from_left_0, from_left_1), (from_right_0, from_right_1)

    grp, fs, tp = lax.axis_index("grp"), lax.axis_index("fs"), lax.axis_index("tp")
    core, chip = lax.rem(tp, 2), lax.div(tp, 2)
    partner, other_core, across = {"grp": 1 - grp}, {"tp": tp + 1 - 2 * core}, {"tp": lax.rem(tp + 2, n_tp)}
    far_tp = lax.rem(tp + 2, n_tp)
    last = n_fs - 1
    at_end = (fs == 0) | (fs == last)
    base = -(-tiles // n_fs)
    short = n_fs * base - tiles
    bf, f32 = jnp.bfloat16, jnp.float32

    def first_tile(dev):
        even = jnp.minimum(dev, short)
        odd = jnp.maximum(dev - (n_fs - short), 0)
        return dev * base - (1 - core) * even - core * odd

    def has_last(dev):
        return first_tile(dev + 1) - first_tile(dev) == base

    def peer(d):
        return lax.rem(fs + d, n_fs)

    def other(j):
        flip = lax.div(2 * fs, n_fs)
        place = fs + flip * (last - 2 * fs)
        o = j + jnp.where(place <= j, 1, 0)
        return o + flip * (last - 2 * o)

    def remote(src, dst, sends, recvs, device):
        return pltpu.make_async_remote_copy(
            src_ref=src, dst_ref=dst, send_sem=sends, recv_sem=recvs, device_id=device, device_id_type=MESH
        )

    def when(cond, fn):
        if cond is None:
            fn()
        else:
            pl.when(cond)(fn)

    def gu_cond(i, dev):
        return has_last(dev) if i // last == base - 1 and short else None

    def gu_z(b, i):
        to, n = other(i % last), i // last
        src = cols[b].at[first_tile(to) + n, grp]
        return remote(src, gu[b].at[n, fs, grp], gu_zs.at[b, i], gu_zr.at[b, n, fs], {"fs": to})

    def gu_landed(b, i):
        o, n = other(i % last), i // last
        block = gu[b].at[n, o, grp]
        return remote(block, block, gu_zs.at[b, i], gu_zr.at[b, n, o], {"fs": o})

    def gu_x(b, i):
        block = gu[b].at[i // last, other(i % last), grp]
        return remote(block, block, gu_xs.at[b, i], gu_xr.at[b, i], partner)

    def dn_part(i):
        return pl.ds(0, base - 1) if i < last else pl.ds(base - 1, 1)

    def dn_cond(i, dev):
        return has_last(dev) if i >= last and short else None

    def dn_z(b, i):
        to = other(i % last)
        start = first_tile(to)
        src = pl.ds(start, base - 1) if i < last else pl.ds(start + base - 1, 1)
        dst = dn[b].at[fs, dn_part(i), grp]
        return remote(rows[b].at[src, grp], dst, dn_zs.at[b, i], dn_zr.at[b, i // last, fs], {"fs": to})

    def dn_landed(b, i):
        o = other(i % last)
        block = dn[b].at[o, dn_part(i), grp]
        return remote(block, block, dn_zs.at[b, i], dn_zr.at[b, i // last, o], {"fs": o})

    def dn_x(b, i):
        block = dn[b].at[other(i % last), dn_part(i), grp]
        return remote(block, block, dn_xs.at[b, i], dn_xr.at[b, i], partner)

    gu_list = [("gu", i) for i in range((n_fs - 1) * base)]
    dn_list = [("dn", i) for i in range((n_fs - 1) * 2)]

    def piece(kind, i):
        if kind == "gu":
            return gu_z, gu_landed, gu_x, gu_cond, i % last
        return dn_z, dn_landed, dn_x, dn_cond, i % last

    def issue(b, pieces):
        for kind, i in pieces:
            along_z, _, _, cond, j = piece(kind, i)
            when(cond(i, other(j)), lambda: along_z(b, i).start())

    def forward(b, pieces):
        for kind, i in pieces:
            _, landed, along_x, cond, _ = piece(kind, i)

            def go():
                landed(b, i).wait_recv()
                along_x(b, i).start()

            when(cond(i, fs), go)

    def collect(b, pieces):
        for kind, i in pieces:
            _, _, along_x, cond, _ = piece(kind, i)
            when(cond(i, fs), lambda: along_x(b, i).wait_recv())

    def drain(b, pieces):
        for kind, i in pieces:
            along_z, _, along_x, cond, j = piece(kind, i)
            when(cond(i, other(j)), lambda: along_z(b, i).wait_send())
            when(cond(i, fs), lambda: along_x(b, i).wait_send())

    def load(b, m):
        dst = (wide_gate, wide_up, wide_down)[m]
        return pltpu.make_async_copy(weights[3 * b + m], dst, load_sem.at[m])

    def cast_columns(b):
        load(b, 0).wait()
        load(b, 1).wait()
        half, step = cols[b].shape[2], 32
        for h in range(2):

            def one(r, carry):
                at = pl.ds(pl.multiple_of(h * half + r * step, step), step)
                to = pl.ds(pl.multiple_of(r * step, step), step)
                for t in range(tiles):
                    lane = pl.ds(t * LANES, LANES)
                    cols[b][t, h, to, :LANES] = wide_gate[at, lane].astype(bf)
                    cols[b][t, h, to, LANES:] = wide_up[at, lane].astype(bf)
                return carry

            lax.fori_loop(0, half // step, one, 0)
        own_tiles(cols[b], lambda n: gu[b].at[n, fs])

    def cast_rows(b):
        load(b, 2).wait()
        half = rows[b].shape[2]

        def one(i, carry):
            at = pl.ds(pl.multiple_of(i * half, half), half)
            rows[b][lax.div(i, 2), lax.rem(i, 2)] = wide_down[at, :].astype(bf)
            return carry

        lax.fori_loop(0, 2 * tiles, one, 0)
        own_tiles(rows[b], lambda n: dn[b].at[fs, n])

    def own_tiles(src, dst):
        start = first_tile(fs)
        for n in range(base):
            def copy():
                dst(n)[...] = src[start + n]

            if n < base - 1 or not short:
                copy()
            else:
                pl.when(has_last(fs))(copy)

    def blank_tiles(b):
        if short:
            @pl.when(jnp.logical_not(has_last(fs)))
            def _():
                gu[b][base - 1] = jnp.zeros(gu[b].shape[1:], bf)
                for a in range(n_fs):
                    dn[b][a, base - 1] = jnp.zeros(dn[b].shape[2:], bf)

    def part(q):
        rows_q = x[0].shape[2] // parts
        return pl.ds(q * rows_q, rows_q)

    def ag_right(b, o, q):
        block = x[b].at[tp, o, part(q)]
        return remote(block, block, ag_zs.at[b, 0, o, q], ag_zr.at[b, o, q], {"fs": peer(1)})

    def ag_left(b, o, q):
        block = x[b].at[tp, o, part(q)]
        return remote(block, block, ag_zs.at[b, 1, o, q], ag_zr.at[b, o, q], {"fs": peer(last)})

    def ag_y(b, o, q, mine=True):
        block = x[b].at[tp if mine else far_tp, o, part(q)]
        return remote(block, block, ag_ys.at[b, o, q], ag_yr.at[b, o, q], across)

    def ag_core(b, o, q, j):
        block = x[b].at[far_tp if j else tp, o, part(q)]
        return remote(block, block, ag_cs.at[b, j, o, q], ag_cr.at[b, j, o, q], other_core)

    def ag_own(b, q):
        pl.when(fs < last)(lambda: ag_right(b, fs, q).start())
        pl.when(fs > 0)(lambda: ag_left(b, fs, q).start())
        ag_y(b, fs, q).start()
        ag_core(b, fs, q, 0).start()

    def ag_hop(b, h):
        for q in range(parts):
            @pl.when(fs - 1 - h >= 0)
            def _():
                o = fs - 1 - h
                ag_right(b, o, q).wait_recv()
                pl.when(fs < last)(lambda: ag_right(b, o, q).start())
                ag_y(b, o, q).start()
                ag_core(b, o, q, 0).start()

            @pl.when(fs + 1 + h <= last)
            def _():
                o = fs + 1 + h
                ag_left(b, o, q).wait_recv()
                pl.when(fs > 0)(lambda: ag_left(b, o, q).start())
                ag_y(b, o, q).start()
                ag_core(b, o, q, 0).start()

    def ag_share(b, o):
        for q in range(parts):
            ag_y(b, o, q, False).wait_recv()
            ag_core(b, o, q, 1).start()

    def ag_share_hop(b, h):
        pl.when(fs - 1 - h >= 0)(lambda: ag_share(b, fs - 1 - h))
        pl.when(fs + 1 + h <= last)(lambda: ag_share(b, fs + 1 + h))

    def ag_arrived(b, o):
        for q in range(parts):
            for j in range(2):
                ag_core(b, o, q, j).wait_recv()

    def ag_drain(b):
        for o in range(n_fs):
            for q in range(parts):
                if o < last:
                    pl.when((fs < last) & (fs >= o))(lambda: ag_right(b, o, q).wait_send())
                if o > 0:
                    pl.when((fs > 0) & (fs <= o))(lambda: ag_left(b, o, q).wait_send())
                ag_y(b, o, q).wait_send()
                for j in range(2):
                    ag_core(b, o, q, j).wait_send()

    def norm(b, k):
        step, width = 64, x[b].shape[3]

        def one(i, carry):
            at = pl.ds(pl.multiple_of(i * step, step), step)
            squares = jnp.zeros((step, width), f32)
            for t in range(n_tp):
                v = x[b][t, k, at, :].astype(f32)
                squares = squares + v * v
            mean = jnp.sum(squares, axis=1, keepdims=True) / (width * n_tp)
            factor = lax.rsqrt(mean + epsilon)
            for t in range(n_tp):
                v = x[b][t, k, at, :].astype(f32) * factor * all_gains[t, b]
                normed[k, at, t * width : (t + 1) * width] = v.astype(bf)
            return carry

        lax.fori_loop(0, x[b].shape[2] // step, one, 0)

    def own_scale(i, n):
        tile = jnp.minimum(first_tile(fs) + n, tiles - 1)
        return scales[i][pl.ds(pl.multiple_of(tile * LANES, LANES), LANES)][None, :]

    def make_hidden(b, k):
        for n in range(base):
            weight = gu[b][n].reshape(-1, 2 * LANES)
            both = jnp.dot(normed[k], weight, preferred_element_type=f32)
            gate = both[:, :LANES] * own_scale(2 * b, n)
            up = both[:, LANES:] * own_scale(2 * b + 1, n)
            value = gate / (1.0 + jnp.exp(-gate)) * up
            hidden[k, :, n * LANES : (n + 1) * LANES] = value.astype(bf)

    def every_block(fn):
        def one(k, carry):
            fn(k)
            return carry

        lax.fori_loop(0, n_fs, one, 0)

    def term(b, a, k):
        weight = dn[b][a].reshape(-1, dn[b].shape[4])
        return jnp.dot(hidden[k], weight, preferred_element_type=f32)

    def rs_core(b, j, k, q):
        src, dst = core_out.at[j, k, part(q)], from_core[b].at[j, k, part(q)]
        return remote(src, dst, rs_cs.at[b, j, k, q], rs_cr.at[b, j, k, q], other_core)

    def rs_y(b, k, q):
        src, dst = y_out.at[k, part(q)], from_y[b].at[k, part(q)]
        return remote(src, dst, rs_ys.at[b, k, q], rs_yr.at[b, k, q], across)

    def rs_right(b, k, q):
        src, dst = z_out.at[k, part(q)], from_left[b].at[k, part(q)]
        return remote(src, dst, rs_zs.at[b, k, q], rs_lr.at[b, k, q], {"fs": peer(1)})

    def rs_left(b, k, q):
        src, dst = z_out.at[k, part(q)], from_right[b].at[k, part(q)]
        return remote(src, dst, rs_zs.at[b, k, q], rs_rr.at[b, k, q], {"fs": peer(last)})

    def turn(kk):
        flip = lax.div(2 * fs, n_fs)
        place = fs + flip * (last - 2 * fs)
        odd, half = lax.rem(kk, 2), lax.div(kk, 2)
        k = jnp.where(place == 0, last - kk, (1 - odd) * (last - half) + odd * half)
        return k + flip * (last - 2 * k)

    def core_stage(b, j, k):
        target = 2 * (1 - chip if j == 0 else chip) + 1 - core
        core_out[j, k] = term(b, target, k).astype(bf)
        for q in range(parts):
            rs_core(b, j, k, q).start()

    def y_stage(b, k):
        total[...] = term(b, far_tp, k)
        for q in range(parts):
            rs_core(b, 0, k, q).wait_recv()
            y_out[k, part(q)] = (total[part(q)] + from_core[b][0, k, part(q)].astype(f32)).astype(bf)
            rs_y(b, k, q).start()

    def z_stage(b, k):
        total[...] = term(b, tp, k)
        for q in range(parts):
            at = part(q)
            rs_core(b, 1, k, q).wait_recv()
            rs_y(b, k, q).wait_recv()
            total[at] = total[at] + from_core[b][1, k, at].astype(f32) + from_y[b][k, at].astype(f32)

            @pl.when((k > fs) & (fs > 0))
            def _():
                rs_right(b, k, q).wait_recv()
                total[at] = total[at] + from_left[b][k, at].astype(f32)

            @pl.when((k < fs) & (fs < last))
            def _():
                rs_left(b, k, q).wait_recv()
                total[at] = total[at] + from_right[b][k, at].astype(f32)

            @pl.when(k == fs)
            def _():
                kept[at] = total[at]

            @pl.when(k != fs)
            def _():
                z_out[k, at] = total[at].astype(bf)

            pl.when(k > fs)(lambda: rs_right(b, k, q).start())
            pl.when(k < fs)(lambda: rs_left(b, k, q).start())

    def z_last(b, finish):
        for q in range(parts):
            at = part(q)

            @pl.when(fs > 0)
            def _():
                rs_right(b, fs, q).wait_recv()
                kept[at] = kept[at] + from_left[b][fs, at].astype(f32)

            @pl.when(fs < last)
            def _():
                rs_left(b, fs, q).wait_recv()
                kept[at] = kept[at] + from_right[b][fs, at].astype(f32)

            value = x[b][tp, fs, at].astype(f32) + 0.5 * kept[at] * down_scales[b]
            finish(q, value.astype(bf))

    def loop(count, fn):
        def one(i, carry):
            fn(i)
            return carry

        lax.fori_loop(0, count, one, 0)

    def scatter(b, hook, finish):
        loop(n_fs, lambda i: core_stage(b, 0, turn(i)))
        hook("core")
        loop(n_fs, lambda i: y_stage(b, turn(i)))
        loop(n_fs, lambda i: core_stage(b, 1, turn(i)))
        for kk in range(n_fs):
            z_stage(b, turn(kk))
            hook(kk)
        z_last(b, finish)

    def scatter_drain(b):
        for k in range(n_fs):
            for q in range(parts):
                for j in range(2):
                    rs_core(b, j, k, q).wait_send()
                rs_y(b, k, q).wait_send()
                pl.when(fs < k)(lambda: rs_right(b, k, q).wait_send())
                pl.when(fs > k)(lambda: rs_left(b, k, q).wait_send())

    own_tokens = pltpu.make_async_copy(tokens, x[0].at[tp, fs], load_sem.at[3])
    own_tokens.start()
    small_loads = []

    def small_load(src, dst):
        small_loads.append(pltpu.make_async_copy(src, dst, small_sem.at[len(small_loads)]))

    for b in range(2):
        gain, gate_s, up_s, down_s = small[4 * b : 4 * b + 4]
        small_load(gain, gains.at[b])
        small_load(down_s, down_scales.at[b])
        small_load(gate_s, scales[2 * b])
        small_load(up_s, scales[2 * b + 1])
    for copy in small_loads:
        copy.start()
    for m in range(3):
        load(0, m).start()

    barrier = pltpu.get_barrier_semaphore()
    greeted = [{"fs": peer(d)} for d in range(1, n_fs)] + [partner]
    greeted = greeted + [{"tp": lax.rem(tp + r, n_tp)} for r in range(1, n_tp)]
    for device in greeted:
        pl.semaphore_signal(barrier, inc=1, device_id=device, device_id_type=MESH)
    pl.semaphore_wait(barrier, len(greeted))

    def gain_copy(r):
        return remote(
            gains, all_gains.at[tp], gain_send.at[r - 1], gain_recv.at[r - 1], {"tp": lax.rem(tp + r, n_tp)}
        )

    own_tokens.wait()
    for q in range(parts):
        ag_own(0, q)
    for copy in small_loads:
        copy.wait()
    for r in range(1, n_tp):
        gain_copy(r).start()
    all_gains[tp] = gains[...]
    for b in range(2):
        blank_tiles(b)
    every = gu_list + dn_list
    count = len(gu_list)
    cast_columns(0)
    issue(0, every[:1])
    cast_rows(0)
    for m in range(3):
        load(1, m).start()
    ag_hop(0, 0)
    issue(0, every[1 : 2 * last])
    ag_share(0, fs)
    cast_columns(1)
    ag_hop(0, 1)
    issue(0, every[2 * last :])
    forward(0, every[:last])
    ag_share_hop(0, 0)
    cast_rows(1)
    forward(0, every[last : 2 * last])
    for h in range(2, last):
        ag_hop(0, h)
    ag_share_hop(0, 1)
    forward(0, every[2 * last : 3 * last - 1])
    for h in range(2, last):
        ag_share_hop(0, h)
    forward(0, every[3 * last - 1 : count])
    pl.when(at_end)(lambda: issue(1, every[:FIRST]))
    for r in range(1, n_tp):
        gain_copy(r).wait_recv()
    for o in range(n_fs):
        ag_arrived(0, o)
    every_block(lambda k: norm(0, k))
    forward(0, every[count : count + 1])
    collect(0, every[:count])
    for k in range(n_fs):
        make_hidden(0, k)
        forward(0, every[count + 1 + k : count + 2 + k])
    forward(0, every[count + 1 + n_fs :])
    pl.when(jnp.logical_not(at_end))(lambda: issue(1, every[:FIRST]))
    collect(0, every[count:])

    sent, passed = [FIRST], [0]

    def hook(stage):
        to_send, to_pass = PLAN.get(stage, (0, 0))
        issue(1, every[sent[0] : to_send])
        sent[0] = max(sent[0], to_send)
        forward(1, every[passed[0] : to_pass])
        passed[0] = max(passed[0], to_pass)

    def pass_on(q, value):
        x[1][tp, fs, part(q)] = value
        ag_own(1, q)

    def ready(k):
        ag_arrived(1, k)
        norm(1, k)
        make_hidden(1, k)

    scatter(0, hook, pass_on)
    hook("own")
    ag_hop(1, 0)
    hook("hop0")
    ag_share(1, fs)
    ag_hop(1, 1)
    hook("hop1")
    ag_share_hop(1, 0)
    collect(1, every[:count])
    ready(fs)
    for h in range(2, last):
        ag_hop(1, h)
        hook("hop%d" % h)
    ag_share_hop(1, 1)
    hook("share1")
    loop(last - 1, lambda i: ready(other(i)))
    scatter_drain(0)
    issue(1, every[sent[0] :])
    forward(1, every[passed[0] :])
    for h in range(2, last):
        ag_share_hop(1, h)
    ready(other(last - 1))
    collect(1, every[count:])

    def put_out(q, value):
        out[part(q)] = value

    scatter(1, lambda stage: None, put_out)
    scatter_drain(1)
    for b in range(2):
        ag_drain(b)
        drain(b, every)
    for r in range(1, n_tp):
        gain_copy(r).wait_send()


def body_kernel(tokens, *rest):
    first, second = rest[:7], rest[7:]
    n_fs, n_tp = lax.axis_size("fs"), lax.axis_size("tp")
    count, feats = tokens.shape
    depth, units = first[1].shape
    tiles = units // LANES
    base = -(-tiles // n_fs)
    half = depth // 2
    bf, f32 = jnp.bfloat16, jnp.float32
    small = []
    for gain, _, gate_s, _, up_s, _, down_s in (first, second):
        small += [gain[None, :], gate_s, up_s, down_s[None, :]]
    weights = [first[1], first[3], first[5], second[1], second[3], second[5]]
    vmem, dma = pltpu.VMEM, pltpu.SemaphoreType.DMA
    any_spec, vmem_spec = pl.BlockSpec(memory_space=pl.ANY), pl.BlockSpec(memory_space=pltpu.VMEM)
    tile = (count, feats)
    scratch = [
        vmem((depth, units), f32), vmem((depth, units), f32), vmem((units, feats), f32),
        vmem((2, 1, feats), f32), vmem((n_tp, 2, 1, feats), f32), vmem((units,), f32), vmem((units,), f32), vmem((units,), f32), vmem((units,), f32), vmem((2, 1, feats), f32),
    ]
    scratch += [vmem((tiles, 2, half, 2 * LANES), bf)] * 2
    scratch += [vmem((tiles, 2, LANES // 2, feats), bf)] * 2
    scratch += [vmem((base, n_fs, 2, half, 2 * LANES), bf)] * 2
    scratch += [vmem((n_fs, base, 2, LANES // 2, feats), bf)] * 2
    scratch += [vmem((n_tp, n_fs, *tile), bf)] * 2
    scratch += [vmem((n_fs, count, n_tp * feats), bf), vmem((n_fs, count, base * LANES), bf)]
    scratch += [vmem((2, n_fs, *tile), bf)] * 3
    scratch += [vmem((n_fs, *tile), bf)] * 3
    scratch += [vmem((n_fs, *tile), bf)] * 5
    scratch += [vmem(tile, f32)] * 2
    scratch += [dma((4,)), dma((8,)), dma((n_tp - 1,)), dma((n_tp - 1,))]
    one, two = dma((2, n_fs, PARTS)), dma((2, 2, n_fs, PARTS))
    scratch += [two, one, one, one, two, two]
    for count_of in (base, 2):
        sent = dma((2, (n_fs - 1) * count_of))
        scratch += [sent, dma((2, count_of, n_fs)), sent, sent]
    scratch += [two] * 2 + [one] * 5
    return pl.pallas_call(
        functools.partial(both_blocks, n_fs, n_tp, tiles, PARTS),
        out_shape=jax.ShapeDtypeStruct(tile, bf),
        in_specs=[any_spec] * 15,
        out_specs=vmem_spec,
        scratch_shapes=scratch,
        compiler_params=pltpu.CompilerParams(
            collective_id=0, has_side_effects=True, vmem_limit_bytes=67043328
        ),
    )(tokens, *small, *weights)


def fits(tokens, *rest):
    n_grp, n_fs, n_tp = (lax.axis_size(name) for name in ("grp", "fs", "tp"))
    depth, units = rest[1].shape
    return (
        n_grp == 2
        and n_fs == n_tp
        and n_tp == 4
        and units % LANES == 0
        and units // LANES > n_fs
        and depth % 64 == 0
        and depth == tokens.shape[1]
        and depth % LANES == 0
        and tokens.shape[0] % 64 == 0
    )


def solution(mesh):
    in_specs = (
        P(("grp", "fs"), "tp"),
        P("tp"),
        P("fs", "tp"),
        P("tp"),
        P("fs", "tp"),
        P("tp"),
        P("tp", "fs"),
        P("tp"),
        P("tp"),
        P("fs", "tp"),
        P("tp"),
        P("fs", "tp"),
        P("tp"),
        P("tp", "fs"),
        P("tp"),
    )
    out_specs = P(("grp", "fs"), "tp")

    def body(*args):
        return (body_kernel if fits(*args) else body_gather)(*args)

    return jax.shard_map(body, mesh=mesh, in_specs=in_specs, out_specs=out_specs, check_vma=False)
```

```python
import functools

import jax
import jax.numpy as jnp
from jax import lax
from jax.experimental import pallas as pl
from jax.experimental.pallas import tpu as pltpu
from jax.sharding import PartitionSpec as P

MESH = pl.DeviceIdType.MESH
LANES = 128
PARTS = 2
FIRST = 7
PLAN = {
    "core": (10, 0),
    0: (11, 3),
    1: (12, 5),
    2: (13, 7),
    3: (13, 9),
    "own": (13, 10),
    "hop0": (15, 12),
    "hop1": (15, 13),
    "hop2": (15, 15),
}

epsilon = 1e-06


def normalize(stream, gain):
    values = stream.astype(jnp.float32)
    totals = lax.psum(jnp.sum(values * values, axis=1), "tp")
    width = values.shape[1] * lax.axis_size("tp")
    normed = (values * lax.rsqrt(totals / width + epsilon)[:, None] * gain).astype(jnp.bfloat16)
    return values, lax.all_gather(normed, "tp", axis=1, tiled=True)


def gathered_block(stream, gain, gate_w, gate_s, up_w, up_s, down_w, down_s):
    values, whole = normalize(stream, gain)

    def project(weight, scale):
        rows = lax.all_gather(weight.astype(jnp.bfloat16), "fs", axis=0, tiled=True)
        return jnp.dot(whole, rows, preferred_element_type=jnp.float32) * scale

    hidden = (jax.nn.silu(project(gate_w, gate_s)) * project(up_w, up_s)).astype(jnp.bfloat16)
    columns = lax.all_gather(down_w.astype(jnp.bfloat16), "fs", axis=1, tiled=True)
    terms = jnp.dot(hidden, columns, preferred_element_type=jnp.float32).astype(jnp.bfloat16)
    summed = lax.psum_scatter(terms, "tp", scatter_dimension=1, tiled=True).astype(jnp.float32)
    return (values + 0.5 * summed * down_s).astype(jnp.bfloat16)


def body_gather(tokens, *rest):
    middle = gathered_block(tokens, *rest[:7])
    return gathered_block(middle, *rest[7:])


def both_blocks(n_fs, n_tp, tiles, parts, *refs):
    tokens, small, weights, out, refs = refs[0], refs[1:9], refs[9:15], refs[15], refs[16:]
    (
        wide_gate, wide_up, wide_down, gains, all_gains, scale_0, scale_1, scale_2, scale_3, down_scales,
        cols_0, cols_1, rows_0, rows_1, gu_0, gu_1, dn_0, dn_1, x_0, x_1, normed, hidden,
        core_out, from_core_0, from_core_1, y_out, from_y_0, from_y_1,
        z_out, from_left_0, from_left_1, from_right_0, from_right_1, total, kept,
        load_sem, small_sem, gain_send, gain_recv,
        ag_zs, ag_zr, ag_ys, ag_yr, ag_cs, ag_cr,
        gu_zs, gu_zr, gu_xs, gu_xr, dn_zs, dn_zr, dn_xs, dn_xr,
        rs_cs, rs_cr, rs_ys, rs_yr, rs_zs, rs_lr, rs_rr,
    ) = refs
    scales = (scale_0, scale_1, scale_2, scale_3)
    cols, rows, gu, dn, x = (cols_0, cols_1), (rows_0, rows_1), (gu_0, gu_1), (dn_0, dn_1), (x_0, x_1)
    from_core, from_y = (from_core_0, from_core_1), (from_y_0, from_y_1)
    from_left, from_right = (from_left_0, from_left_1), (from_right_0, from_right_1)

    grp, fs, tp = lax.axis_index("grp"), lax.axis_index("fs"), lax.axis_index("tp")
    core, chip = lax.rem(tp, 2), lax.div(tp, 2)
    partner, other_core, across = {"grp": 1 - grp}, {"tp": tp + 1 - 2 * core}, {"tp": lax.rem(tp + 2, n_tp)}
    far_tp = lax.rem(tp + 2, n_tp)
    last = n_fs - 1
    at_end = (fs == 0) | (fs == last)
    base = -(-tiles // n_fs)
    short = n_fs * base - tiles
    bf, f32 = jnp.bfloat16, jnp.float32

    def first_tile(dev):
        even = jnp.minimum(dev, short)
        odd = jnp.maximum(dev - (n_fs - short), 0)
        return dev * base - (1 - core) * even - core * odd

    def has_last(dev):
        return first_tile(dev + 1) - first_tile(dev) == base

    def peer(d):
        return lax.rem(fs + d, n_fs)

    def other(j):
        flip = lax.div(2 * fs, n_fs)
        place = fs + flip * (last - 2 * fs)
        o = j + jnp.where(place <= j, 1, 0)
        return o + flip * (last - 2 * o)

    def remote(src, dst, sends, recvs, device):
        return pltpu.make_async_remote_copy(
            src_ref=src, dst_ref=dst, send_sem=sends, recv_sem=recvs, device_id=device, device_id_type=MESH
        )

    def when(cond, fn):
        if cond is None:
            fn()
        else:
            pl.when(cond)(fn)

    def gu_cond(i, dev):
        return has_last(dev) if i // last == base - 1 and short else None

    def gu_z(b, i):
        to, n = other(i % last), i // last
        src = cols[b].at[first_tile(to) + n, grp]
        return remote(src, gu[b].at[n, fs, grp], gu_zs.at[b, i], gu_zr.at[b, n, fs], {"fs": to})

    def gu_landed(b, i):
        o, n = other(i % last), i // last
        block = gu[b].at[n, o, grp]
        return remote(block, block, gu_zs.at[b, i], gu_zr.at[b, n, o], {"fs": o})

    def gu_x(b, i):
        block = gu[b].at[i // last, other(i % last), grp]
        return remote(block, block, gu_xs.at[b, i], gu_xr.at[b, i], partner)

    def dn_part(i):
        return pl.ds(0, base - 1) if i < last else pl.ds(base - 1, 1)

    def dn_cond(i, dev):
        return has_last(dev) if i >= last and short else None

    def dn_z(b, i):
        to = other(i % last)
        start = first_tile(to)
        src = pl.ds(start, base - 1) if i < last else pl.ds(start + base - 1, 1)
        dst = dn[b].at[fs, dn_part(i), grp]
        return remote(rows[b].at[src, grp], dst, dn_zs.at[b, i], dn_zr.at[b, i // last, fs], {"fs": to})

    def dn_landed(b, i):
        o = other(i % last)
        block = dn[b].at[o, dn_part(i), grp]
        return remote(block, block, dn_zs.at[b, i], dn_zr.at[b, i // last, o], {"fs": o})

    def dn_x(b, i):
        block = dn[b].at[other(i % last), dn_part(i), grp]
        return remote(block, block, dn_xs.at[b, i], dn_xr.at[b, i], partner)

    gu_list = [("gu", i) for i in range((n_fs - 1) * base)]
    dn_list = [("dn", i) for i in range((n_fs - 1) * 2)]

    def piece(kind, i):
        if kind == "gu":
            return gu_z, gu_landed, gu_x, gu_cond, i % last
        return dn_z, dn_landed, dn_x, dn_cond, i % last

    def issue(b, pieces):
        for kind, i in pieces:
            along_z, _, _, cond, j = piece(kind, i)
            when(cond(i, other(j)), lambda: along_z(b, i).start())

    def forward(b, pieces):
        for kind, i in pieces:
            _, landed, along_x, cond, _ = piece(kind, i)

            def go():
                landed(b, i).wait_recv()
                along_x(b, i).start()

            when(cond(i, fs), go)

    def collect(b, pieces):
        for kind, i in pieces:
            _, _, along_x, cond, _ = piece(kind, i)
            when(cond(i, fs), lambda: along_x(b, i).wait_recv())

    def drain(b, pieces):
        for kind, i in pieces:
            along_z, _, along_x, cond, j = piece(kind, i)
            when(cond(i, other(j)), lambda: along_z(b, i).wait_send())
            when(cond(i, fs), lambda: along_x(b, i).wait_send())

    def load(b, m):
        dst = (wide_gate, wide_up, wide_down)[m]
        return pltpu.make_async_copy(weights[3 * b + m], dst, load_sem.at[m])

    def cast_columns(b):
        load(b, 0).wait()
        load(b, 1).wait()
        half, step = cols[b].shape[2], 32
        for h in range(2):

            def one(r, carry):
                at = pl.ds(pl.multiple_of(h * half + r * step, step), step)
                to = pl.ds(pl.multiple_of(r * step, step), step)
                for t in range(tiles):
                    lane = pl.ds(t * LANES, LANES)
                    cols[b][t, h, to, :LANES] = wide_gate[at, lane].astype(bf)
                    cols[b][t, h, to, LANES:] = wide_up[at, lane].astype(bf)
                return carry

            lax.fori_loop(0, half // step, one, 0)
        own_tiles(cols[b], lambda n: gu[b].at[n, fs])

    def cast_rows(b):
        load(b, 2).wait()
        half = rows[b].shape[2]

        def one(i, carry):
            at = pl.ds(pl.multiple_of(i * half, half), half)
            rows[b][lax.div(i, 2), lax.rem(i, 2)] = wide_down[at, :].astype(bf)
            return carry

        lax.fori_loop(0, 2 * tiles, one, 0)
        own_tiles(rows[b], lambda n: dn[b].at[fs, n])

    def own_tiles(src, dst):
        start = first_tile(fs)
        for n in range(base):
            def copy():
                dst(n)[...] = src[start + n]

            if n < base - 1 or not short:
                copy()
            else:
                pl.when(has_last(fs))(copy)

    def blank_tiles(b):
        if short:
            @pl.when(jnp.logical_not(has_last(fs)))
            def _():
                gu[b][base - 1] = jnp.zeros(gu[b].shape[1:], bf)
                for a in range(n_fs):
                    dn[b][a, base - 1] = jnp.zeros(dn[b].shape[2:], bf)

    def part(q):
        rows_q = x[0].shape[2] // parts
        return pl.ds(q * rows_q, rows_q)

    def ag_right(b, o, q):
        block = x[b].at[tp, o, part(q)]
        return remote(block, block, ag_zs.at[b, 0, o, q], ag_zr.at[b, o, q], {"fs": peer(1)})

    def ag_left(b, o, q):
        block = x[b].at[tp, o, part(q)]
        return remote(block, block, ag_zs.at[b, 1, o, q], ag_zr.at[b, o, q], {"fs": peer(last)})

    def ag_y(b, o, q, mine=True):
        block = x[b].at[tp if mine else far_tp, o, part(q)]
        return remote(block, block, ag_ys.at[b, o, q], ag_yr.at[b, o, q], across)

    def ag_core(b, o, q, j):
        block = x[b].at[far_tp if j else tp, o, part(q)]
        return remote(block, block, ag_cs.at[b, j, o, q], ag_cr.at[b, j, o, q], other_core)

    def ag_own(b, q):
        pl.when(fs < last)(lambda: ag_right(b, fs, q).start())
        pl.when(fs > 0)(lambda: ag_left(b, fs, q).start())
        ag_y(b, fs, q).start()
        ag_core(b, fs, q, 0).start()

    def ag_hop(b, h):
        for q in range(parts):
            @pl.when(fs - 1 - h >= 0)
            def _():
                o = fs - 1 - h
                ag_right(b, o, q).wait_recv()
                pl.when(fs < last)(lambda: ag_right(b, o, q).start())
                ag_y(b, o, q).start()
                ag_core(b, o, q, 0).start()

            @pl.when(fs + 1 + h <= last)
            def _():
                o = fs + 1 + h
                ag_left(b, o, q).wait_recv()
                pl.when(fs > 0)(lambda: ag_left(b, o, q).start())
                ag_y(b, o, q).start()
                ag_core(b, o, q, 0).start()

    def ag_share(b, o):
        for q in range(parts):
            ag_y(b, o, q, False).wait_recv()
            ag_core(b, o, q, 1).start()

    def ag_share_hop(b, h):
        pl.when(fs - 1 - h >= 0)(lambda: ag_share(b, fs - 1 - h))
        pl.when(fs + 1 + h <= last)(lambda: ag_share(b, fs + 1 + h))

    def ag_arrived(b, o):
        for q in range(parts):
            for j in range(2):
                ag_core(b, o, q, j).wait_recv()

    def ag_drain(b):
        for o in range(n_fs):
            for q in range(parts):
                if o < last:
                    pl.when((fs < last) & (fs >= o))(lambda: ag_right(b, o, q).wait_send())
                if o > 0:
                    pl.when((fs > 0) & (fs <= o))(lambda: ag_left(b, o, q).wait_send())
                ag_y(b, o, q).wait_send()
                for j in range(2):
                    ag_core(b, o, q, j).wait_send()

    def norm(b, k):
        step, width = 64, x[b].shape[3]

        def one(i, carry):
            at = pl.ds(pl.multiple_of(i * step, step), step)
            squares = jnp.zeros((step, width), f32)
            for t in range(n_tp):
                v = x[b][t, k, at, :].astype(f32)
                squares = squares + v * v
            mean = jnp.sum(squares, axis=1, keepdims=True) / (width * n_tp)
            factor = lax.rsqrt(mean + epsilon)
            for t in range(n_tp):
                v = x[b][t, k, at, :].astype(f32) * factor * all_gains[t, b]
                normed[k, at, t * width : (t + 1) * width] = v.astype(bf)
            return carry

        lax.fori_loop(0, x[b].shape[2] // step, one, 0)

    def own_scale(i, n):
        tile = jnp.minimum(first_tile(fs) + n, tiles - 1)
        return scales[i][pl.ds(pl.multiple_of(tile * LANES, LANES), LANES)][None, :]

    def make_hidden(b, k):
        for n in range(base):
            weight = gu[b][n].reshape(-1, 2 * LANES)
            both = jnp.dot(normed[k], weight, preferred_element_type=f32)
            gate = both[:, :LANES] * own_scale(2 * b, n)
            up = both[:, LANES:] * own_scale(2 * b + 1, n)
            value = gate / (1.0 + jnp.exp(-gate)) * up
            hidden[k, :, n * LANES : (n + 1) * LANES] = value.astype(bf)

    def every_block(fn):
        def one(k, carry):
            fn(k)
            return carry

        lax.fori_loop(0, n_fs, one, 0)

    def term(b, a, k):
        weight = dn[b][a].reshape(-1, dn[b].shape[4])
        return jnp.dot(hidden[k], weight, preferred_element_type=f32)

    def rs_core(b, j, k, q):
        src, dst = core_out.at[j, k, part(q)], from_core[b].at[j, k, part(q)]
        return remote(src, dst, rs_cs.at[b, j, k, q], rs_cr.at[b, j, k, q], other_core)

    def rs_y(b, k, q):
        src, dst = y_out.at[k, part(q)], from_y[b].at[k, part(q)]
        return remote(src, dst, rs_ys.at[b, k, q], rs_yr.at[b, k, q], across)

    def rs_right(b, k, q):
        src, dst = z_out.at[k, part(q)], from_left[b].at[k, part(q)]
        return remote(src, dst, rs_zs.at[b, k, q], rs_lr.at[b, k, q], {"fs": peer(1)})

    def rs_left(b, k, q):
        src, dst = z_out.at[k, part(q)], from_right[b].at[k, part(q)]
        return remote(src, dst, rs_zs.at[b, k, q], rs_rr.at[b, k, q], {"fs": peer(last)})

    def turn(kk):
        flip = lax.div(2 * fs, n_fs)
        place = fs + flip * (last - 2 * fs)
        odd, half = lax.rem(kk, 2), lax.div(kk, 2)
        k = jnp.where(place == 0, last - kk, (1 - odd) * (last - half) + odd * half)
        return k + flip * (last - 2 * k)

    def core_stage(b, j, k):
        target = 2 * (1 - chip if j == 0 else chip) + 1 - core
        core_out[j, k] = term(b, target, k).astype(bf)
        for q in range(parts):
            rs_core(b, j, k, q).start()

    def y_stage(b, k):
        total[...] = term(b, far_tp, k)
        for q in range(parts):
            rs_core(b, 0, k, q).wait_recv()
            y_out[k, part(q)] = (total[part(q)] + from_core[b][0, k, part(q)].astype(f32)).astype(bf)
            rs_y(b, k, q).start()

    def z_stage(b, k):
        total[...] = term(b, tp, k)
        for q in range(parts):
            rs_core(b, 1, k, q).wait_recv()
            total[part(q)] = total[part(q)] + from_core[b][1, k, part(q)].astype(f32)
        for q in range(parts):
            at = part(q)
            rs_y(b, k, q).wait_recv()
            total[at] = total[at] + from_y[b][k, at].astype(f32)

            @pl.when((k > fs) & (fs > 0))
            def _():
                rs_right(b, k, q).wait_recv()
                total[at] = total[at] + from_left[b][k, at].astype(f32)

            @pl.when((k < fs) & (fs < last))
            def _():
                rs_left(b, k, q).wait_recv()
                total[at] = total[at] + from_right[b][k, at].astype(f32)

            @pl.when(k == fs)
            def _():
                kept[at] = total[at]

            @pl.when(k != fs)
            def _():
                z_out[k, at] = total[at].astype(bf)

            pl.when(k > fs)(lambda: rs_right(b, k, q).start())
            pl.when(k < fs)(lambda: rs_left(b, k, q).start())

    def z_last(b, finish):
        for q in range(parts):
            at = part(q)

            @pl.when(fs > 0)
            def _():
                rs_right(b, fs, q).wait_recv()
                kept[at] = kept[at] + from_left[b][fs, at].astype(f32)

            @pl.when(fs < last)
            def _():
                rs_left(b, fs, q).wait_recv()
                kept[at] = kept[at] + from_right[b][fs, at].astype(f32)

            value = x[b][tp, fs, at].astype(f32) + 0.5 * kept[at] * down_scales[b]
            finish(q, value.astype(bf))

    def loop(count, fn):
        def one(i, carry):
            fn(i)
            return carry

        lax.fori_loop(0, count, one, 0)

    def scatter(b, hook, finish):
        core_stage(b, 0, turn(0))
        hook("core")

        def ahead(i):
            pl.when(i < last)(lambda: core_stage(b, 0, turn(i + 1)))
            y_stage(b, turn(i))

        loop(n_fs, ahead)
        loop(n_fs, lambda i: core_stage(b, 1, turn(i)))
        for kk in range(n_fs):
            z_stage(b, turn(kk))
            hook(kk)
        z_last(b, finish)

    def scatter_drain(b):
        for k in range(n_fs):
            for q in range(parts):
                for j in range(2):
                    rs_core(b, j, k, q).wait_send()
                rs_y(b, k, q).wait_send()
                pl.when(fs < k)(lambda: rs_right(b, k, q).wait_send())
                pl.when(fs > k)(lambda: rs_left(b, k, q).wait_send())

    own_tokens = pltpu.make_async_copy(tokens, x[0].at[tp, fs], load_sem.at[3])
    own_tokens.start()
    small_loads = []

    def small_load(src, dst):
        small_loads.append(pltpu.make_async_copy(src, dst, small_sem.at[len(small_loads)]))

    for b in range(2):
        gain, gate_s, up_s, down_s = small[4 * b : 4 * b + 4]
        small_load(gain, gains.at[b])
        small_load(down_s, down_scales.at[b])
        small_load(gate_s, scales[2 * b])
        small_load(up_s, scales[2 * b + 1])
    for copy in small_loads:
        copy.start()
    for m in range(3):
        load(0, m).start()

    barrier = pltpu.get_barrier_semaphore()
    greeted = [{"fs": peer(d)} for d in range(1, n_fs)] + [partner]
    greeted = greeted + [{"tp": lax.rem(tp + r, n_tp)} for r in range(1, n_tp)]
    for device in greeted:
        pl.semaphore_signal(barrier, inc=1, device_id=device, device_id_type=MESH)
    pl.semaphore_wait(barrier, len(greeted))

    def gain_copy(r):
        return remote(
            gains, all_gains.at[tp], gain_send.at[r - 1], gain_recv.at[r - 1], {"tp": lax.rem(tp + r, n_tp)}
        )

    own_tokens.wait()
    for q in range(parts):
        ag_own(0, q)
    for copy in small_loads:
        copy.wait()
    for r in range(1, n_tp):
        gain_copy(r).start()
    all_gains[tp] = gains[...]
    for b in range(2):
        blank_tiles(b)
    every = gu_list + dn_list
    count = len(gu_list)
    cast_columns(0)
    issue(0, every[:1])
    cast_rows(0)
    for m in range(3):
        load(1, m).start()
    ag_hop(0, 0)
    issue(0, every[1 : 2 * last])
    ag_share(0, fs)
    cast_columns(1)
    ag_hop(0, 1)
    issue(0, every[2 * last :])
    forward(0, every[:last])
    ag_share_hop(0, 0)
    cast_rows(1)
    forward(0, every[last : 2 * last])
    for h in range(2, last):
        ag_hop(0, h)
    ag_share_hop(0, 1)
    forward(0, every[2 * last : 3 * last - 1])
    for h in range(2, last):
        ag_share_hop(0, h)
    forward(0, every[3 * last - 1 : count])
    pl.when(at_end)(lambda: issue(1, every[:FIRST]))
    for r in range(1, n_tp):
        gain_copy(r).wait_recv()
    for o in range(n_fs):
        ag_arrived(0, o)
    every_block(lambda k: norm(0, k))
    forward(0, every[count : count + 1])
    collect(0, every[:count])
    for k in range(n_fs):
        make_hidden(0, k)
        forward(0, every[count + 1 + k : count + 2 + k])
    forward(0, every[count + 1 + n_fs :])
    pl.when(jnp.logical_not(at_end))(lambda: issue(1, every[:FIRST]))
    collect(0, every[count:])

    sent, passed = [FIRST], [0]

    def hook(stage):
        to_send, to_pass = PLAN.get(stage, (0, 0))
        issue(1, every[sent[0] : to_send])
        sent[0] = max(sent[0], to_send)
        forward(1, every[passed[0] : to_pass])
        passed[0] = max(passed[0], to_pass)

    def pass_on(q, value):
        x[1][tp, fs, part(q)] = value
        ag_own(1, q)

    def ready(k):
        ag_arrived(1, k)
        norm(1, k)
        make_hidden(1, k)

    scatter(0, hook, pass_on)
    hook("own")
    ag_hop(1, 0)
    hook("hop0")
    ag_share(1, fs)
    ag_hop(1, 1)
    hook("hop1")
    ag_share_hop(1, 0)
    collect(1, every[:count])
    ready(fs)
    for h in range(2, last):
        ag_hop(1, h)
        hook("hop%d" % h)
    ag_share_hop(1, 1)
    hook("share1")
    loop(last - 1, lambda i: ready(other(i)))
    scatter_drain(0)
    issue(1, every[sent[0] :])
    forward(1, every[passed[0] :])
    for h in range(2, last):
        ag_share_hop(1, h)
    ready(other(last - 1))
    collect(1, every[count:])

    def put_out(q, value):
        out[part(q)] = value

    scatter(1, lambda stage: None, put_out)
    scatter_drain(1)
    for b in range(2):
        ag_drain(b)
        drain(b, every)
    for r in range(1, n_tp):
        gain_copy(r).wait_send()


def body_kernel(tokens, *rest):
    first, second = rest[:7], rest[7:]
    n_fs, n_tp = lax.axis_size("fs"), lax.axis_size("tp")
    count, feats = tokens.shape
    depth, units = first[1].shape
    tiles = units // LANES
    base = -(-tiles // n_fs)
    half = depth // 2
    bf, f32 = jnp.bfloat16, jnp.float32
    small = []
    for gain, _, gate_s, _, up_s, _, down_s in (first, second):
        small += [gain[None, :], gate_s, up_s, down_s[None, :]]
    weights = [first[1], first[3], first[5], second[1], second[3], second[5]]
    vmem, dma = pltpu.VMEM, pltpu.SemaphoreType.DMA
    any_spec, vmem_spec = pl.BlockSpec(memory_space=pl.ANY), pl.BlockSpec(memory_space=pltpu.VMEM)
    tile = (count, feats)
    scratch = [
        vmem((depth, units), f32), vmem((depth, units), f32), vmem((units, feats), f32),
        vmem((2, 1, feats), f32), vmem((n_tp, 2, 1, feats), f32), vmem((units,), f32), vmem((units,), f32), vmem((units,), f32), vmem((units,), f32), vmem((2, 1, feats), f32),
    ]
    scratch += [vmem((tiles, 2, half, 2 * LANES), bf)] * 2
    scratch += [vmem((tiles, 2, LANES // 2, feats), bf)] * 2
    scratch += [vmem((base, n_fs, 2, half, 2 * LANES), bf)] * 2
    scratch += [vmem((n_fs, base, 2, LANES // 2, feats), bf)] * 2
    scratch += [vmem((n_tp, n_fs, *tile), bf)] * 2
    scratch += [vmem((n_fs, count, n_tp * feats), bf), vmem((n_fs, count, base * LANES), bf)]
    scratch += [vmem((2, n_fs, *tile), bf)] * 3
    scratch += [vmem((n_fs, *tile), bf)] * 3
    scratch += [vmem((n_fs, *tile), bf)] * 5
    scratch += [vmem(tile, f32)] * 2
    scratch += [dma((4,)), dma((8,)), dma((n_tp - 1,)), dma((n_tp - 1,))]
    one, two = dma((2, n_fs, PARTS)), dma((2, 2, n_fs, PARTS))
    scratch += [two, one, one, one, two, two]
    for count_of in (base, 2):
        sent = dma((2, (n_fs - 1) * count_of))
        scratch += [sent, dma((2, count_of, n_fs)), sent, sent]
    scratch += [two] * 2 + [one] * 5
    return pl.pallas_call(
        functools.partial(both_blocks, n_fs, n_tp, tiles, PARTS),
        out_shape=jax.ShapeDtypeStruct(tile, bf),
        in_specs=[any_spec] * 15,
        out_specs=vmem_spec,
        scratch_shapes=scratch,
        compiler_params=pltpu.CompilerParams(
            collective_id=0, has_side_effects=True, vmem_limit_bytes=67043328
        ),
    )(tokens, *small, *weights)


def fits(tokens, *rest):
    n_grp, n_fs, n_tp = (lax.axis_size(name) for name in ("grp", "fs", "tp"))
    depth, units = rest[1].shape
    return (
        n_grp == 2
        and n_fs == n_tp
        and n_tp == 4
        and units % LANES == 0
        and units // LANES > n_fs
        and depth % 64 == 0
        and depth == tokens.shape[1]
        and depth % LANES == 0
        and tokens.shape[0] % 64 == 0
    )


def solution(mesh):
    in_specs = (
        P(("grp", "fs"), "tp"),
        P("tp"),
        P("fs", "tp"),
        P("tp"),
        P("fs", "tp"),
        P("tp"),
        P("tp", "fs"),
        P("tp"),
        P("tp"),
        P("fs", "tp"),
        P("tp"),
        P("fs", "tp"),
        P("tp"),
        P("tp", "fs"),
        P("tp"),
    )
    out_specs = P(("grp", "fs"), "tp")

    def body(*args):
        return (body_kernel if fits(*args) else body_gather)(*args)

    return jax.shard_map(body, mesh=mesh, in_specs=in_specs, out_specs=out_specs, check_vma=False)
```
